32 devices in a mesh: grp: 2 (over y), sp: 4 (over z), tp: 4 (over x, core).
Axes of the slice: x: 2, y: 2, z: 4, core: 2. Of those that a mesh axis runs over, the one named last changes fastest.
Arguments:
- tokens: bfloat16 [1024, 2048], P(('grp', 'sp')), parts along dimension 0, may hold values from -8 to 8
- norm_gain: float32 [2048], replicated, may hold values from 0.1 to 1.9
- w_query: bfloat16 [2048, 1024], P(None, 'tp'), may hold values from -0.125 to 0.125
- w_key: bfloat16 [2048, 1024], P(None, 'tp'), may hold values from -0.125 to 0.125
- w_value: bfloat16 [2048, 1024], P(None, 'tp'), may hold values from -0.125 to 0.125
- w_out: bfloat16 [1024, 2048], P('tp'), may hold values from -0.1875 to 0.1875
- key_rate: bfloat16 [16, 1024], P('tp', ('grp', 'sp')), parts along dimension 1, may hold values from -16 to 1
Outputs:
- layer_out: bfloat16 [1024, 2048], P(('grp', 'sp')), parts along dimension 0
The draws below stay inside these ranges and needn't reach their ends.
There are 2 independent parts, one for each index of `grp`. The reference program is written for one: setup_inputs(seed, part) draws one part's arguments, and reference() takes and returns one part's arrays. A program takes and returns all parts, laid end to end along the dimension named above; an argument that names none is the same for every part. Nothing has to cross between parts.
All inputs are finite; a program needn't handle non-finite values.
Results may differ from the reference program's by a relative error of at most 0.0075.
Values may be sent and summed in bfloat16 or wider, within the bound.
No kernel may reach another device: no remote copies, remote signals or barrier semaphores. Data moves between devices by JAX's collectives and lax.ppermute only.
A program may use at most 64 MiB of HBM per device.

```python
import jax
import jax.numpy as jnp
from jax import lax

D = 2048
HEAD_TOTAL = 16
HD = 64
KEY_SPAN = 128
TOK_DEV = 128
TOKEN_TOTAL = 512


def draw_tokens(key, part):
    noise_key, offset_key = jax.random.split(jax.random.fold_in(key, 3))
    block_count = TOKEN_TOTAL // TOK_DEV
    base_draw = jax.random.normal(noise_key, (TOKEN_TOTAL, D), jnp.float32)
    offsets = 0.8 * jax.random.normal(offset_key, (block_count, D), jnp.float32)
    drawn_rows = base_draw + jnp.repeat(offsets, TOK_DEV, axis=0)
    return jnp.clip(drawn_rows, -8.0, 8.0).astype(jnp.bfloat16)


def draw_key_rate(key, part):
    random_subkeys = jax.random.split(jax.random.fold_in(key, 7), 7)
    block_count = TOKEN_TOTAL // TOK_DEV
    slow_share = 0.5
    slow_heads = jax.random.uniform(random_subkeys[0], (HEAD_TOTAL,), jnp.float32) < slow_share
    log_length = jnp.log(jnp.float32(TOKEN_TOTAL))
    slow_rate = -log_length + jax.random.uniform(random_subkeys[1], (HEAD_TOTAL,), jnp.float32, -1.0, 0.3)
    fast_rate = jax.random.uniform(random_subkeys[2], (HEAD_TOTAL,), jnp.float32, -4.5, -3.0)
    head_rate = jnp.where(slow_heads, slow_rate, fast_rate)
    block_term = jax.random.uniform(random_subkeys[3], (HEAD_TOTAL, block_count), jnp.float32, -0.7, 0.7)
    rough = 0.3 * jax.random.normal(random_subkeys[4], (HEAD_TOTAL, TOKEN_TOTAL), jnp.float32)
    spike_position = jax.random.randint(random_subkeys[5], (4,), 0, TOKEN_TOTAL)
    spike_level = jax.random.uniform(random_subkeys[6], (HEAD_TOTAL, 4), jnp.float32, -1.5, 0.0)
    token_positions = jnp.arange(TOKEN_TOTAL, dtype=jnp.int32)
    match_count = token_positions[None, :] == spike_position[:, None]
    spike_value = jnp.einsum('me,eq->mq', spike_level, match_count.astype(jnp.float32))
    spike_flag = jnp.any(match_count, axis=0)
    rate_row_values = head_rate[:, None] + jnp.repeat(block_term, TOK_DEV, axis=1) + rough
    rate_row_values = jnp.where(spike_flag[None, :], spike_value, rate_row_values)
    return jnp.clip(rate_row_values, -16.0, 1.0).astype(jnp.bfloat16)


def levels(own_key, dims, cuts, low, high):
    gain = 1.0
    for axis_at, shards_of in cuts:
        heights = jax.random.uniform(jax.random.fold_in(jax.random.fold_in(own_key, 6), axis_at), (shards_of,), jnp.float32, low / len(cuts), high / len(cuts))
        gain = gain * jnp.repeat(jnp.exp(heights), dims[axis_at] // shards_of).reshape((-1,) + (1,) * (len(dims) - 1 - axis_at))
    return gain


def centred(rng, extent, spread, limit, pieces=(), kind=jnp.bfloat16):
    level = levels(rng, extent, pieces, -0.22, 0.18) if pieces else 1.0
    array = jax.random.normal(rng, extent, jnp.float32) * spread * level
    return jnp.minimum(jnp.maximum(array, -limit), limit).astype(kind)


def setup_inputs(seed: int = 0, part: int = 0) -> dict:
    key_list = jax.random.split(jax.random.key(seed), 8)
    own_keys = jax.random.split(jax.random.fold_in(key_list[7], part), 8)
    return {
        "tokens": draw_tokens(jax.random.fold_in(jax.random.fold_in(key_list[7], part), 71), part),
        "norm_gain": jnp.clip(1.0 + 0.18 * jax.random.normal(key_list[1], (D,), jnp.float32), 0.1, 1.9),
        "w_query": centred(key_list[2], (D, HEAD_TOTAL * HD), D ** -0.5, 0.125, ((1, 4),)),
        "w_key": centred(key_list[3], (D, HEAD_TOTAL * HD), D ** -0.5, 0.125, ((1, 4),)),
        "w_value": centred(key_list[4], (D, HEAD_TOTAL * HD), D ** -0.5, 0.125, ((1, 4),)),
        "w_out": centred(key_list[5], (HEAD_TOTAL * HD, D), (HEAD_TOTAL * HD) ** -0.5, 0.1875, ((0, 4),)),
        "key_rate": draw_key_rate(jax.random.fold_in(jax.random.fold_in(key_list[7], part), 71), part),
    }


F32 = jnp.float32
BF16 = jnp.bfloat16
HIGHEST = lax.Precision.HIGHEST
EPS = 1e-06

def shard_summary(query_heads, key_heads, value_heads, rate_row_values, query_pos, key_pos):
    scores = jnp.einsum('qhd,khd->hqk', query_heads.astype(F32), key_heads.astype(F32)) * HD ** (-0.5)
    scores = scores + jnp.transpose(rate_row_values).astype(F32)[:, None, :]
    causal_mask = key_pos[None, :] < query_pos[:, None]
    log_remain = jnp.where(causal_mask[None], jax.nn.log_sigmoid(-scores), 0.0)
    heads_here, query_count, key_count = scores.shape
    span_count = key_count // KEY_SPAN
    blocks = log_remain.reshape(heads_here, query_count, span_count, KEY_SPAN)
    span_ids = jnp.arange(KEY_SPAN, dtype=jnp.int32)
    tri_strict = (span_ids[:, None] > span_ids[None, :]).astype(F32)
    inside_sum = jnp.einsum('hqnj,js->hqns', blocks, tri_strict, precision=HIGHEST)
    block_ids = jnp.arange(span_count, dtype=jnp.int32)
    block_later = (block_ids[:, None] > block_ids[None, :]).astype(F32)
    beyond = jnp.einsum('hqn,nm->hqm', lax.optimization_barrier(jnp.sum(blocks, axis=-1)), block_later, precision=HIGHEST)
    suffix = (inside_sum + beyond[..., None]).reshape(heads_here, query_count, key_count)
    weight = jnp.where(causal_mask[None], jnp.exp(jax.nn.log_sigmoid(scores) + suffix), 0.0).astype(BF16)
    weight = lax.optimization_barrier(weight).astype(F32)
    partial_value = jnp.einsum('hqk,khd->qhd', weight, value_heads.astype(F32))
    return (partial_value.reshape(query_count, heads_here * HD), lax.optimization_barrier(jnp.sum(log_remain, axis=-1)))

def reference(tokens, norm_gain, w_query, w_key, w_value, w_out, key_rate):
    tokens_f = tokens.astype(F32)
    normed = (tokens_f * lax.rsqrt(lax.optimization_barrier(jnp.mean(tokens_f * tokens_f, axis=-1, keepdims=True)) + EPS) * norm_gain).astype(BF16)
    queries = lax.optimization_barrier(jnp.dot(normed, w_query, preferred_element_type=F32).astype(BF16))
    key_rows = lax.optimization_barrier(jnp.dot(normed, w_key, preferred_element_type=F32).astype(BF16))
    value_rows = lax.optimization_barrier(jnp.dot(normed, w_value, preferred_element_type=F32).astype(BF16))
    shard_total = TOKEN_TOTAL // TOK_DEV
    query_shards = queries.reshape(shard_total, TOK_DEV, HEAD_TOTAL, HD)
    key_shards = key_rows.reshape(shard_total, TOK_DEV, HEAD_TOTAL, HD)
    value_shards = value_rows.reshape(shard_total, TOK_DEV, HEAD_TOTAL, HD)
    rate_shards = jnp.transpose(key_rate).reshape(shard_total, TOK_DEV, HEAD_TOTAL)
    local_pos = jnp.arange(TOK_DEV, dtype=jnp.int32)
    shard_ids = jnp.arange(shard_total, dtype=jnp.int32)
    later_mask = (shard_ids[:, None] > shard_ids[None, :]).astype(F32)

    def one_shard(item_tuple):
        query_index, query_heads = item_tuple
        query_pos = query_index * TOK_DEV + local_pos

        def absorb_one(state_pair, key_tuple):
            key_index, key_heads, value_heads, rate_row_values = key_tuple
            empty_pair = (jnp.zeros((TOK_DEV, HEAD_TOTAL * HD), F32), jnp.zeros((HEAD_TOTAL, TOK_DEV), F32))
            result = lax.cond(key_index <= query_index, lambda: shard_summary(query_heads, key_heads, value_heads, rate_row_values, query_pos, key_index * TOK_DEV + local_pos), lambda: empty_pair)
            return (state_pair, result)
        _, (partials, remains) = lax.scan(absorb_one, None, (shard_ids, key_shards, value_shards, rate_shards))
        beyond = jnp.einsum('nhq,nm->mhq', remains, later_mask, precision=HIGHEST)
        factor = jnp.transpose(jnp.exp(beyond), (0, 2, 1))[..., None]
        mixed_rows = lax.optimization_barrier(jnp.sum(partials.reshape(shard_total, TOK_DEV, HEAD_TOTAL, HD) * factor, axis=0))
        return mixed_rows.reshape(TOK_DEV, HEAD_TOTAL * HD).astype(BF16)
    mixed = lax.map(one_shard, (shard_ids, query_shards)).reshape(TOKEN_TOTAL, HEAD_TOTAL * HD)
    return jnp.dot(mixed, w_out, preferred_element_type=F32).astype(BF16)
```

```python
import functools

import jax
import jax.numpy as jnp
from jax import lax
from jax.experimental import pallas as pl
from jax.experimental.pallas import tpu as pltpu
from jax.sharding import PartitionSpec as P

HD = 64
EPS = 1e-06
F32 = jnp.float32
BF16 = jnp.bfloat16
VMEM_SPEC = pl.BlockSpec(memory_space=pltpu.VMEM)
HBM_SPEC = pl.BlockSpec(memory_space=pltpu.HBM)


def project_kernel(chunks, tok_hbm, gain_ref, rate_ref, wk_hbm, wv_hbm, wq_hbm, kv_ref, q_ref, tok, w, normed, tok_sem, w_sem):
    rows, model = tok.shape
    width = q_ref.shape[1]
    depth = model // chunks
    tok_copy = pltpu.make_async_copy(tok_hbm, tok, tok_sem)
    tok_copy.start()
    copies = []
    for i, ref in enumerate((wk_hbm, wv_hbm, wq_hbm)):
        for c in range(chunks):
            copy = pltpu.make_async_copy(
                ref.at[pl.ds(c * depth, depth)], w.at[i, pl.ds(c * depth, depth)], w_sem.at[i, c]
            )
            copy.start()
            copies.append(copy)
    tok_copy.wait()
    values = tok[...].astype(F32)
    scale = lax.rsqrt(jnp.mean(values * values, axis=-1, keepdims=True) + EPS)
    normed[...] = (values * scale * gain_ref[...]).astype(BF16)
    for i in range(3):
        total = jnp.zeros((rows, width), F32)
        for c in range(chunks):
            copies[i * chunks + c].wait()
            total += jnp.dot(
                normed[:, pl.ds(c * depth, depth)],
                w[i, pl.ds(c * depth, depth)],
                preferred_element_type=F32,
            )
        out = total.astype(BF16)
        if i < 2:
            kv_ref[pl.ds(0, rows), pl.ds(i * width, width)] = out
        else:
            q_ref[...] = out * jnp.asarray(HD**-0.5, BF16)
    pad = jnp.zeros((kv_ref.shape[0] - rows, 2 * width), BF16)
    kv_ref[pl.ds(rows, kv_ref.shape[0] - rows), :] = pad
    heads = rate_ref.shape[0]
    kv_ref[pl.ds(rows, heads), pl.ds(0, rows)] = rate_ref[...]


def project(tokens, gain, rate, w_key, w_value, w_query):
    rows, model = tokens.shape
    width = w_query.shape[1]
    chunks = 4
    rate_rows = -(-rate.shape[0] // 8) * 8
    return pl.pallas_call(
        functools.partial(project_kernel, chunks),
        out_shape=(
            jax.ShapeDtypeStruct((rows + rate_rows, 2 * width), BF16),
            jax.ShapeDtypeStruct((rows, width), BF16),
        ),
        in_specs=[HBM_SPEC, VMEM_SPEC, VMEM_SPEC, HBM_SPEC, HBM_SPEC, HBM_SPEC],
        out_specs=(VMEM_SPEC, VMEM_SPEC),
        scratch_shapes=[
            pltpu.VMEM((rows, model), BF16),
            pltpu.VMEM((3, model, width), BF16),
            pltpu.VMEM((rows, model), BF16),
            pltpu.SemaphoreType.DMA,
            pltpu.SemaphoreType.DMA((3, chunks)),
        ],
        cost_estimate=pl.CostEstimate(flops=6 * rows * model * width, bytes_accessed=6 * model * width, transcendentals=0),
        compiler_params=pltpu.CompilerParams(vmem_limit_bytes=8 << 20),
        name="project",
    )(tokens, gain.reshape(1, model), rate, w_key, w_value, w_query)


def attend_kernel(diagonal, q_ref, kv_ref, *refs):
    if diagonal:
        acc_out, rest_out = refs
    else:
        acc_in, rest_in, acc_out, rest_out = refs
    rows, width = q_ref.shape
    heads = width // HD
    q = q_ref[...]
    lane = lax.broadcasted_iota(jnp.int32, (rows, width), 1) // HD
    stacked = jnp.concatenate([jnp.where(lane == h, q, jnp.zeros_like(q)) for h in range(heads)], axis=0)
    keys = kv_ref[pl.ds(0, rows), pl.ds(0, width)]
    values = kv_ref[pl.ds(0, rows), pl.ds(width, width)]
    scores = lax.dot_general(stacked, keys, (((1,), (1,)), ((), ())), preferred_element_type=F32)
    rate = kv_ref[pl.ds(rows, heads), pl.ds(0, rows)].astype(F32)
    scores = jnp.concatenate(
        [scores[h * rows : (h + 1) * rows] + rate[h : h + 1] for h in range(heads)], axis=0
    )
    softened = jnp.log(1.0 + jnp.exp(-jnp.abs(scores)))
    log_keep = jnp.minimum(scores, 0.0) - softened
    log_remain = -jnp.maximum(scores, 0.0) - softened
    if diagonal:
        q_pos = lax.broadcasted_iota(jnp.int32, (heads * rows, rows), 0) % rows
        k_pos = lax.broadcasted_iota(jnp.int32, (heads * rows, rows), 1)
        mask = k_pos < q_pos
        log_remain = jnp.where(mask, log_remain, 0.0)
    high = log_remain.astype(BF16)
    low = (log_remain - high.astype(F32)).astype(BF16)
    from_pos = lax.broadcasted_iota(jnp.int32, (2 * rows, 2 * rows), 0) % rows
    to_pos = lax.broadcasted_iota(jnp.int32, (2 * rows, 2 * rows), 1)
    later = ((from_pos > to_pos) | (to_pos >= rows)).astype(F32).astype(BF16)
    sums = jnp.dot(jnp.concatenate([high, low], axis=1), later, preferred_element_type=F32)
    exponent = log_keep + sums[:, :rows]
    rest = sums[:, rows:]
    if not diagonal:
        exponent = exponent + rest_in[...]
        rest = rest + rest_in[...]
    weight = jnp.exp(exponent)
    if diagonal:
        weight = jnp.where(mask, weight, 0.0)
    weight = weight.astype(BF16)
    spread = jnp.dot(weight, values, preferred_element_type=F32)
    acc = jnp.zeros((rows, width), F32) if diagonal else acc_in[...]
    for h in range(heads):
        acc = acc + jnp.where(lane == h, spread[h * rows : (h + 1) * rows], 0.0)
    acc_out[...] = acc.astype(acc_out.dtype)
    rest_out[...] = rest


def attend(q, kv, state, last):
    rows, width = q.shape
    heads = width // HD
    diagonal = state is None
    operands = (q, kv) if diagonal else (q, kv, *state)
    return pl.pallas_call(
        functools.partial(attend_kernel, diagonal),
        out_shape=(
            jax.ShapeDtypeStruct((rows, width), BF16 if last else F32),
            jax.ShapeDtypeStruct((heads * rows, rows), F32),
        ),
        in_specs=[VMEM_SPEC] * len(operands),
        out_specs=(VMEM_SPEC, VMEM_SPEC),
        cost_estimate=pl.CostEstimate(flops=1000000000, bytes_accessed=1000000, transcendentals=0),
        compiler_params=pltpu.CompilerParams(vmem_limit_bytes=8 << 20),
        name="attend",
    )(*operands)


def output_kernel(count, *refs):
    out_ref = refs[-1]
    total = jnp.zeros(out_ref.shape, F32)
    for i in range(count):
        total += jnp.dot(refs[i][...], refs[count + i][...], preferred_element_type=F32)
    out_ref[...] = total.astype(BF16)


def output(mixed, weights):
    rows = mixed[0].shape[0]
    model = weights[0].shape[1]
    count = len(mixed)
    block = 512
    return pl.pallas_call(
        functools.partial(output_kernel, count),
        grid=(model // block,),
        out_shape=jax.ShapeDtypeStruct((rows, model), BF16),
        in_specs=[pl.BlockSpec(m.shape, lambda j: (0, 0)) for m in mixed]
        + [pl.BlockSpec((w.shape[0], block), lambda j: (0, j)) for w in weights],
        out_specs=pl.BlockSpec((rows, block), lambda j: (0, j)),
        cost_estimate=pl.CostEstimate(flops=2000000000, bytes_accessed=4000000, transcendentals=0),
        compiler_params=pltpu.CompilerParams(vmem_limit_bytes=12 << 20),
        name="output",
    )(*mixed, *weights)


def on_device(tokens, norm_gain, w_query, w_key, w_value, w_out, key_rate):
    shards = lax.axis_size("sp")
    group = lax.axis_size("tp")

    def swap(x, bit):
        return lax.ppermute(x, "tp", [(i, i ^ bit) for i in range(group)])

    bits = []
    while 2 << len(bits) <= group:
        bits.append(1 << len(bits))
    bits = bits[::-1]
    weights = [w_out]
    for bit in bits[:-1]:
        weights = weights + [swap(w, bit) for w in weights]
    near = swap(w_out, bits[-1])

    kv, q = project(tokens, norm_gain, key_rate, w_key, w_value, w_query)
    arrived = [
        lax.ppermute(kv, "sp", [(i, i + d) for i in range(shards - d)]) for d in range(1, shards)
    ]
    state = attend(q, kv, None, shards == 1)
    for d, block in enumerate(arrived):
        state = attend(q, block, state, d == shards - 2)
    mixed = [state[0]]
    weights += [near] + [swap(lax.optimization_barrier((w, state[0]))[0], bits[-1]) for w in weights[1:]]
    for bit in bits:
        joined = mixed[0] if len(mixed) == 1 else jnp.concatenate(mixed, axis=1)
        other = swap(joined, bit)
        width = mixed[0].shape[1]
        mixed = mixed + [other[:, i * width : (i + 1) * width] for i in range(len(mixed))]
    return output(mixed, weights)


def solution(mesh):
    return jax.shard_map(
        on_device,
        mesh=mesh,
        in_specs=(
            P(("grp", "sp"), None),
            P(),
            P(None, "tp"),
            P(None, "tp"),
            P(None, "tp"),
            P("tp", None),
            P("tp", ("grp", "sp")),
        ),
        out_specs=P(("grp", "sp"), None),
        check_vma=False,
    )
```

```python
import functools

import jax
import jax.numpy as jnp
from jax import lax
from jax.experimental import pallas as pl
from jax.experimental.pallas import tpu as pltpu
from jax.sharding import PartitionSpec as P

HD = 64
EPS = 1e-06
F32 = jnp.float32
BF16 = jnp.bfloat16
VMEM_SPEC = pl.BlockSpec(memory_space=pltpu.VMEM)
HBM_SPEC = pl.BlockSpec(memory_space=pltpu.HBM)


def in_hbm(x):
    return pltpu.with_memory_space_constraint(x, pltpu.HBM)


def params(mib):
    return pltpu.CompilerParams(vmem_limit_bytes=mib << 20)


def cost(flops):
    return pl.CostEstimate(flops=flops, bytes_accessed=1 << 20, transcendentals=0)


def project_kernel(chunks, tok_hbm, gain_hbm, rate_hbm, wk_hbm, wv_hbm, wq_hbm, kv_ref, q_ref, kq_ref, tok, gain, rate, w, normed, sems, w_sems):
    rows, model = tok.shape
    width = q_ref.shape[1]
    heads = rate.shape[0]
    depth = model // chunks
    small = []
    for i, (src, dst) in enumerate(((tok_hbm, tok), (gain_hbm, gain), (rate_hbm, rate))):
        small.append(pltpu.make_async_copy(src, dst, sems.at[i]))
        small[-1].start()
    copies = []
    for i, ref in enumerate((wk_hbm, wv_hbm, wq_hbm)):
        for c in range(chunks):
            span = pl.ds(c * depth, depth)
            copies.append(pltpu.make_async_copy(ref.at[span], w.at[i, span], w_sems.at[i, c]))
            copies[-1].start()
    for copy in small:
        copy.wait()
    extra = kv_ref.shape[0] - rows
    for ref in (kv_ref, kq_ref):
        ref[pl.ds(rows, extra), :] = jnp.zeros((extra, 2 * width), BF16)
        ref[pl.ds(rows, heads), pl.ds(0, rows)] = rate[...]
    values = tok[...].astype(F32)
    scale = lax.rsqrt(jnp.mean(values * values, axis=-1, keepdims=True) + EPS)
    normed[...] = (values * scale * gain[...]).astype(BF16)
    for i in range(3):
        total = jnp.zeros((rows, width), F32)
        for c in range(chunks):
            span = pl.ds(c * depth, depth)
            copies[i * chunks + c].wait()
            total += jnp.dot(normed[:, span], w[i, span], preferred_element_type=F32)
        out = total.astype(BF16)
        if i < 2:
            kv_ref[pl.ds(0, rows), pl.ds(i * width, width)] = out
        if i == 0:
            kq_ref[pl.ds(0, rows), pl.ds(0, width)] = out
        if i == 2:
            out = out * jnp.asarray(HD**-0.5, BF16)
            q_ref[...] = out
            kq_ref[pl.ds(0, rows), pl.ds(width, width)] = out


def project(tokens, gain, rate, w_key, w_value, w_query):
    rows, model = tokens.shape
    width = w_query.shape[1]
    chunks = 4
    packed = jax.ShapeDtypeStruct((rows + -(-rate.shape[0] // 8) * 8, 2 * width), BF16)
    operands = (tokens, gain.reshape(1, model), rate, w_key, w_value, w_query)
    return pl.pallas_call(
        functools.partial(project_kernel, chunks),
        out_shape=(packed, jax.ShapeDtypeStruct((rows, width), BF16), packed),
        in_specs=[HBM_SPEC] * 6,
        out_specs=(VMEM_SPEC,) * 3,
        scratch_shapes=[
            pltpu.VMEM((rows, model), BF16),
            pltpu.VMEM((1, model), F32),
            pltpu.VMEM(rate.shape, BF16),
            pltpu.VMEM((3, model, width), BF16),
            pltpu.VMEM((rows, model), BF16),
            pltpu.SemaphoreType.DMA((3,)),
            pltpu.SemaphoreType.DMA((3, chunks)),
        ],
        cost_estimate=cost(6 * rows * model * width),
        compiler_params=params(8),
        name="project",
    )(*(in_hbm(x) for x in operands))


def lanes_of(rows, width):
    return lax.broadcasted_iota(jnp.int32, (rows, width), 1) // HD


def stack_heads(q):
    rows, width = q.shape
    lane = lanes_of(rows, width)
    return jnp.concatenate([jnp.where(lane == h, q, jnp.zeros_like(q)) for h in range(width // HD)], axis=0)


def unstack_heads(spread, rows):
    width = spread.shape[1]
    lane = lanes_of(rows, width)
    total = jnp.zeros((rows, width), F32)
    for h in range(width // HD):
        total = total + jnp.where(lane == h, spread[h * rows : (h + 1) * rows], 0.0)
    return total


def later_matrix(rows):
    start = lax.broadcasted_iota(jnp.int32, (2 * rows, 2 * rows), 0) % rows
    stop = lax.broadcasted_iota(jnp.int32, (2 * rows, 2 * rows), 1)
    return ((start > stop) | (stop >= rows)).astype(F32).astype(BF16)


def logs(stacked, packed, later, diagonal):
    rows = later.shape[0] // 2
    width = stacked.shape[1]
    heads = width // HD
    keys = packed[pl.ds(0, rows), pl.ds(0, width)]
    rate = packed[pl.ds(rows, heads), pl.ds(0, rows)].astype(F32)
    scores = lax.dot_general(stacked, keys, (((1,), (1,)), ((), ())), preferred_element_type=F32)
    scores = jnp.concatenate([scores[h * rows : (h + 1) * rows] + rate[h : h + 1] for h in range(heads)], axis=0)
    softened = jnp.log(1.0 + jnp.exp(-jnp.abs(scores)))
    log_keep = jnp.minimum(scores, 0.0) - softened
    log_remain = -jnp.maximum(scores, 0.0) - softened
    mask = None
    if diagonal:
        q_pos = lax.broadcasted_iota(jnp.int32, scores.shape, 0) % rows
        k_pos = lax.broadcasted_iota(jnp.int32, scores.shape, 1)
        mask = k_pos < q_pos
        log_remain = jnp.where(mask, log_remain, 0.0)
    high = log_remain.astype(BF16)
    low = (log_remain - high.astype(F32)).astype(BF16)
    sums = jnp.dot(jnp.concatenate([high, low], axis=1), later, preferred_element_type=F32)
    return log_keep, sums[:, :rows], sums[:, rows:], mask


def absorb(stacked, packed, later, rest, diagonal=False):
    rows = later.shape[0] // 2
    width = stacked.shape[1]
    log_keep, inside, whole, mask = logs(stacked, packed, later, diagonal)
    exponent = log_keep + inside
    if rest is not None:
        exponent = exponent + rest
        whole = whole + rest
    weight = jnp.exp(exponent)
    if diagonal:
        weight = jnp.where(mask, weight, 0.0)
    values = packed[pl.ds(0, rows), pl.ds(width, width)]
    spread = jnp.dot(weight.astype(BF16), values, preferred_element_type=F32)
    return unstack_heads(spread, rows), whole


def own_kernel(q_ref, kv_ref, acc_ref, rest_ref):
    rows = q_ref.shape[0]
    acc_ref[...], rest_ref[...] = absorb(stack_heads(q_ref[...]), kv_ref, later_matrix(rows), None, True)


def ahead_kernel(kq_ref, own_ref, kv_ref, q_ref, acc_ref, rest_ref):
    rows = acc_ref.shape[0]
    width = kq_ref.shape[1] // 2
    q = kq_ref[pl.ds(0, rows), pl.ds(width, width)]
    q_ref[...] = q
    stacked = stack_heads(q)
    later = later_matrix(rows)
    rest = logs(stacked, kq_ref, later, True)[2] + logs(stacked, own_ref, later, False)[2]
    acc_ref[...], rest_ref[...] = absorb(stacked, kv_ref, later, rest)


def more_kernel(sets, last, kv_ref, *refs):
    ins, outs = refs[: 3 * sets], refs[3 * sets :]
    per = 1 if last else 2
    rows = ins[0].shape[0]
    later = later_matrix(rows)
    for i in range(sets):
        q_ref, acc_ref, rest_ref = ins[3 * i : 3 * i + 3]
        acc, rest = absorb(stack_heads(q_ref[...]), kv_ref, later, rest_ref[...])
        acc = acc + acc_ref[...]
        outs[per * i][...] = acc.astype(outs[per * i].dtype)
        if not last:
            outs[per * i + 1][...] = rest


def state_shapes(q, last=False):
    rows, width = q.shape
    if last:
        return (jax.ShapeDtypeStruct((rows, width), BF16),)
    return (
        jax.ShapeDtypeStruct((rows, width), F32),
        jax.ShapeDtypeStruct((width // HD * rows, rows), F32),
    )


def local_call(kernel, name, flops, out_shape, *operands):
    return pl.pallas_call(
        kernel,
        out_shape=out_shape,
        in_specs=[VMEM_SPEC] * len(operands),
        out_specs=(VMEM_SPEC,) * len(out_shape),
        cost_estimate=cost(flops),
        compiler_params=params(12),
        name=name,
    )(*operands)


def own_block(q, kv):
    return (q, *local_call(own_kernel, "own", 600000000, state_shapes(q), q, kv))


def ahead_blocks(kq, own, kv, q):
    shapes = (jax.ShapeDtypeStruct(q.shape, BF16), *state_shapes(q))
    return local_call(ahead_kernel, "ahead", 1200000000, shapes, kq, own, kv)


def more_block(kv, states, last):
    q = states[0][0]
    sets = len(states)
    flat = [x for state in states for x in state]
    out = local_call(
        functools.partial(more_kernel, sets, last), "more", 600000000 * sets, state_shapes(q, last) * sets, kv, *flat
    )
    if last:
        return list(out)
    return [(states[i][0], out[2 * i], out[2 * i + 1]) for i in range(sets)]


def output_kernel(count, parts, block, *refs):
    mixed, weights = refs[:count], refs[count : count + sum(parts)]
    out_hbm, staged, sems = refs[count + sum(parts) :]
    rows, model = staged.shape
    depth = weights[0].shape[0]
    copies = []
    for j in range(0, model, block):
        columns = pl.ds(j, block)
        total = jnp.zeros((rows, block), F32)
        at = 0
        for i in range(count):
            for k in range(parts[i]):
                left = mixed[i][:, pl.ds(k * depth, depth)]
                total += jnp.dot(left, weights[at][:, columns], preferred_element_type=F32)
                at += 1
        staged[:, columns] = total.astype(BF16)
        copies.append(pltpu.make_async_copy(staged.at[:, columns], out_hbm.at[:, columns], sems.at[j // block]))
        copies[-1].start()
    for copy in copies:
        copy.wait()


def output(mixed, weights):
    rows = mixed[0].shape[0]
    depth, model = weights[0].shape
    parts = tuple(m.shape[1] // depth for m in mixed)
    block = 512 if model % 512 == 0 else model
    return pl.pallas_call(
        functools.partial(output_kernel, len(mixed), parts, block),
        out_shape=jax.ShapeDtypeStruct((rows, model), BF16),
        in_specs=[VMEM_SPEC] * (len(mixed) + len(weights)),
        out_specs=HBM_SPEC,
        scratch_shapes=[pltpu.VMEM((rows, model), BF16), pltpu.SemaphoreType.DMA((model // block,))],
        cost_estimate=cost(2 * rows * depth * len(weights) * model),
        compiler_params=params(8),
        name="output",
    )(*mixed, *weights)


def on_device(tokens, norm_gain, w_query, w_key, w_value, w_out, key_rate):
    shards = lax.axis_size("sp")
    group = lax.axis_size("tp")
    bits = []
    while 2 << len(bits) <= group:
        bits.append(1 << len(bits))
    bits = bits[::-1]

    def swap(x, bit):
        return lax.ppermute(x, "tp", [(i, i ^ bit) for i in range(group)])

    weights = [w_out]
    for bit in bits[:-1]:
        weights = weights + [swap(w, bit) for w in weights]
    weight_core = swap(w_out, bits[-1])

    kv, q, kq = project(tokens, norm_gain, key_rate, w_key, w_value, w_query)
    split = shards > 2
    behind = range(1, shards - 1 if split else shards)
    arrived = []
    for d in behind:
        stop = shards if d == 1 else behind[-1] + 1
        arrived.append(lax.ppermute(kv, "sp", [(i, i + d) for i in range(stop - d)]))
    if split:
        kq = lax.ppermute(kq, "sp", [(shards - 1, shards - 2)])
    states = [own_block(q, kv)]
    for i, block in enumerate(arrived):
        last = i == len(arrived) - 1
        if i == 0 and split:
            if last:
                near = more_block(block, states, True)
                far = ahead_blocks(kq, kv, block, q)
                states = near + [far[1].astype(BF16)]
            else:
                states = more_block(block, states, False) + [tuple(ahead_blocks(kq, kv, block, q))]
        else:
            states = more_block(block, states, last)
    if not arrived:
        states = [states[0][1].astype(BF16)]
    near = states[0]

    if split:
        far = states[1]
        same = lax.ppermute(far, "sp", [(shards - 2, shards - 1)])
    if split and len(bits) == 2:
        crossed = lax.ppermute(
            far,
            ("sp", "tp"),
            [((shards - 2) * group + i, (shards - 1) * group + (i ^ bits[0])) for i in range(group)],
        )
        near_x = swap(near, bits[0])
        mixed = jnp.concatenate([near + same, near_x + crossed], axis=1)
    else:
        mixed = near + same if split else near
        for bit in bits[:-1]:
            mixed = jnp.concatenate([mixed, swap(mixed, bit)], axis=1)
    weights = (
        weights
        + [weight_core]
        + [swap(lax.optimization_barrier((w, mixed))[0], bits[-1]) for w in weights[1:]]
    )
    return output([mixed, swap(mixed, bits[-1])], weights)


def solution(mesh):
    return jax.shard_map(
        on_device,
        mesh=mesh,
        in_specs=(
            P(("grp", "sp"), None),
            P(),
            P(None, "tp"),
            P(None, "tp"),
            P(None, "tp"),
            P("tp", None),
            P("tp", ("grp", "sp")),
        ),
        out_specs=P(("grp", "sp"), None),
        check_vma=False,
    )
```

```python
import functools

import jax
import jax.numpy as jnp
from jax import lax
from jax.experimental import pallas as pl
from jax.experimental.pallas import tpu as pltpu
from jax.sharding import PartitionSpec as P


HD = 64
EPS = 1e-06
F32 = jnp.float32
BF16 = jnp.bfloat16
VMEM_SPEC = pl.BlockSpec(memory_space=pltpu.VMEM)
HBM_SPEC = pl.BlockSpec(memory_space=pltpu.HBM)


def in_hbm(x):
    return pltpu.with_memory_space_constraint(x, pltpu.HBM)


def params(mib):
    return pltpu.CompilerParams(vmem_limit_bytes=mib << 20)


def cost(flops):
    return pl.CostEstimate(flops=flops, bytes_accessed=1 << 20, transcendentals=0)


def load_and_multiply(left, sources, held, sems, chunks, emit):
    model = left.shape[1]
    depth = model // chunks
    copies = []
    for i, source in enumerate(sources):
        for c in range(chunks):
            span = pl.ds(c * depth, depth)
            copies.append(pltpu.make_async_copy(source.at[span], held.at[i, span], sems.at[i, c]))
            copies[-1].start()

    def run():
        for i in range(len(sources)):
            total = jnp.zeros((left.shape[0], held.shape[2]), F32)
            for c in range(chunks):
                span = pl.ds(c * depth, depth)
                copies[i * chunks + c].wait()
                total += jnp.dot(left[:, span], held[i, span], preferred_element_type=F32)
            emit(i, total.astype(BF16))

    return run


def key_value_kernel(chunks, tok_hbm, gain_hbm, rate_hbm, wk_hbm, wv_hbm, kv_ref, normed, tok, gain, rate, held, sems, w_sems):
    rows, _ = tok.shape
    width = held.shape[2]
    heads = rate.shape[0]
    small = []
    for i, (src, dst) in enumerate(((tok_hbm, tok), (gain_hbm, gain), (rate_hbm, rate))):
        small.append(pltpu.make_async_copy(src, dst, sems.at[i]))
        small[-1].start()

    def emit(i, out):
        kv_ref[pl.ds(0, rows), pl.ds(i * width, width)] = out

    run = load_and_multiply(normed, (wk_hbm, wv_hbm), held, w_sems, chunks, emit)
    for copy in small:
        copy.wait()
    extra = kv_ref.shape[0] - rows
    kv_ref[pl.ds(rows, extra), :] = jnp.zeros((extra, 2 * width), BF16)
    kv_ref[pl.ds(rows, heads), pl.ds(0, rows)] = rate[...]
    values = tok[...].astype(F32)
    scale = lax.rsqrt(jnp.mean(values * values, axis=-1, keepdims=True) + EPS)
    normed[...] = (values * scale * gain[...]).astype(BF16)
    run()


def query_kernel(chunks, normed, kv_ref, wq_hbm, q_ref, kq_ref, held, w_sems):
    rows, width = q_ref.shape

    def emit(i, out):
        out = out * jnp.asarray(HD**-0.5, BF16)
        q_ref[...] = out
        kq_ref[pl.ds(0, rows), pl.ds(width, width)] = out

    run = load_and_multiply(normed, (wq_hbm,), held, w_sems, chunks, emit)
    extra = kq_ref.shape[0] - rows
    kq_ref[pl.ds(0, rows), pl.ds(0, width)] = kv_ref[pl.ds(0, rows), pl.ds(0, width)]
    kq_ref[pl.ds(rows, extra), :] = kv_ref[pl.ds(rows, extra), :]
    run()


def key_values(tokens, gain, rate, w_key, w_value):
    rows, model = tokens.shape
    width = w_key.shape[1]
    chunks = 4
    packed = jax.ShapeDtypeStruct((rows + -(-rate.shape[0] // 8) * 8, 2 * width), BF16)
    operands = (tokens, gain.reshape(1, model), rate, w_key, w_value)
    return pl.pallas_call(
        functools.partial(key_value_kernel, chunks),
        out_shape=(packed, jax.ShapeDtypeStruct((rows, model), BF16)),
        in_specs=[HBM_SPEC] * 5,
        out_specs=(VMEM_SPEC,) * 2,
        scratch_shapes=[
            pltpu.VMEM((rows, model), BF16),
            pltpu.VMEM((1, model), F32),
            pltpu.VMEM(rate.shape, BF16),
            pltpu.VMEM((2, model, width), BF16),
            pltpu.SemaphoreType.DMA((3,)),
            pltpu.SemaphoreType.DMA((2, chunks)),
        ],
        cost_estimate=cost(4 * rows * model * width),
        compiler_params=params(8),
        name="keyvalue",
    )(*(in_hbm(x) for x in operands))


def queries(normed, kv, w_query):
    rows, model = normed.shape
    width = w_query.shape[1]
    chunks = 4
    return pl.pallas_call(
        functools.partial(query_kernel, chunks),
        out_shape=(jax.ShapeDtypeStruct((rows, width), BF16), jax.ShapeDtypeStruct(kv.shape, BF16)),
        in_specs=[VMEM_SPEC, VMEM_SPEC, HBM_SPEC],
        out_specs=(VMEM_SPEC,) * 2,
        scratch_shapes=[pltpu.VMEM((1, model, width), BF16), pltpu.SemaphoreType.DMA((1, chunks))],
        cost_estimate=cost(2 * rows * model * width),
        compiler_params=params(8),
        name="query",
    )(normed, kv, in_hbm(w_query))


def lanes_of(rows, width):
    return lax.broadcasted_iota(jnp.int32, (rows, width), 1) // HD


def stack_heads(q):
    rows, width = q.shape
    lane = lanes_of(rows, width)
    return jnp.concatenate([jnp.where(lane == h, q, jnp.zeros_like(q)) for h in range(width // HD)], axis=0)


def unstack_heads(spread, rows):
    width = spread.shape[1]
    lane = lanes_of(rows, width)
    total = jnp.zeros((rows, width), F32)
    for h in range(width // HD):
        total = total + jnp.where(lane == h, spread[h * rows : (h + 1) * rows], 0.0)
    return total


def later_matrix(rows):
    start = lax.broadcasted_iota(jnp.int32, (2 * rows, 2 * rows), 0) % rows
    stop = lax.broadcasted_iota(jnp.int32, (2 * rows, 2 * rows), 1)
    return ((start > stop) | (stop >= rows)).astype(F32).astype(BF16)


def logs(stacked, packed, later, diagonal):
    rows = later.shape[0] // 2
    width = stacked.shape[1]
    heads = width // HD
    keys = packed[pl.ds(0, rows), pl.ds(0, width)]
    rate = packed[pl.ds(rows, heads), pl.ds(0, rows)].astype(F32)
    scores = lax.dot_general(stacked, keys, (((1,), (1,)), ((), ())), preferred_element_type=F32)
    scores = jnp.concatenate([scores[h * rows : (h + 1) * rows] + rate[h : h + 1] for h in range(heads)], axis=0)
    softened = jnp.log(1.0 + jnp.exp(-jnp.abs(scores)))
    log_keep = jnp.minimum(scores, 0.0) - softened
    log_remain = -jnp.maximum(scores, 0.0) - softened
    mask = None
    if diagonal:
        q_pos = lax.broadcasted_iota(jnp.int32, scores.shape, 0) % rows
        k_pos = lax.broadcasted_iota(jnp.int32, scores.shape, 1)
        mask = k_pos < q_pos
        log_remain = jnp.where(mask, log_remain, 0.0)
    high = log_remain.astype(BF16)
    low = (log_remain - high.astype(F32)).astype(BF16)
    sums = jnp.dot(jnp.concatenate([high, low], axis=1), later, preferred_element_type=F32)
    return log_keep, sums[:, :rows], sums[:, rows:], mask


def absorb(stacked, packed, later, rest, diagonal=False):
    rows = later.shape[0] // 2
    width = stacked.shape[1]
    log_keep, inside, whole, mask = logs(stacked, packed, later, diagonal)
    exponent = log_keep + inside
    if rest is not None:
        exponent = exponent + rest
        whole = whole + rest
    weight = jnp.exp(exponent)
    if diagonal:
        weight = jnp.where(mask, weight, 0.0)
    values = packed[pl.ds(0, rows), pl.ds(width, width)]
    spread = jnp.dot(weight.astype(BF16), values, preferred_element_type=F32)
    return unstack_heads(spread, rows), whole


def own_kernel(q_ref, kv_ref, acc_ref, rest_ref):
    rows = q_ref.shape[0]
    acc_ref[...], rest_ref[...] = absorb(stack_heads(q_ref[...]), kv_ref, later_matrix(rows), None, True)


def ahead_kernel(kq_ref, own_ref, kv_ref, q_ref, acc_ref, rest_ref):
    rows = acc_ref.shape[0]
    width = kq_ref.shape[1] // 2
    q = kq_ref[pl.ds(0, rows), pl.ds(width, width)]
    q_ref[...] = q
    stacked = stack_heads(q)
    later = later_matrix(rows)
    rest = logs(stacked, kq_ref, later, True)[2] + logs(stacked, own_ref, later, False)[2]
    acc_ref[...], rest_ref[...] = absorb(stacked, kv_ref, later, rest)


def more_kernel(sets, last, reach, kv_ref, *refs):
    ins, outs = refs[: 3 * sets], refs[3 * sets :]
    per = 1 if last else 2
    rows = ins[0].shape[0]
    later = later_matrix(rows)
    for i in range(sets):
        q_ref, acc_ref, rest_ref = ins[3 * i : 3 * i + 3]
        acc, rest = absorb(stack_heads(q_ref[...]), kv_ref, later, rest_ref[...])
        if reach:
            acc = jnp.where(lax.axis_index("sp") >= reach, acc, 0.0)
        acc = acc + acc_ref[...]
        outs[per * i][...] = acc.astype(outs[per * i].dtype)
        if not last:
            outs[per * i + 1][...] = rest


def state_shapes(q, last=False):
    rows, width = q.shape
    if last:
        return (jax.ShapeDtypeStruct((rows, width), BF16),)
    return (
        jax.ShapeDtypeStruct((rows, width), F32),
        jax.ShapeDtypeStruct((width // HD * rows, rows), F32),
    )


def local_call(kernel, flops, out_shape, *operands):
    return pl.pallas_call(
        kernel,
        out_shape=out_shape,
        in_specs=[VMEM_SPEC] * len(operands),
        out_specs=(VMEM_SPEC,) * len(out_shape),
        cost_estimate=cost(flops),
        compiler_params=params(12),
    )(*operands)


def own_block(q, kv):
    return (q, *local_call(own_kernel, 600000000, state_shapes(q), q, kv))


def ahead_blocks(kq, own, kv, q):
    shapes = (jax.ShapeDtypeStruct(q.shape, BF16), *state_shapes(q))
    return local_call(ahead_kernel, 1200000000, shapes, kq, own, kv)


def more_block(kv, states, last, reach):
    q = states[0][0]
    sets = len(states)
    flat = [x for state in states for x in state]
    out = local_call(
        functools.partial(more_kernel, sets, last, reach), 600000000 * sets, state_shapes(q, last) * sets, kv, *flat
    )
    if last:
        return list(out)
    return [(states[i][0], out[2 * i], out[2 * i + 1]) for i in range(sets)]


def output_kernel(plan, block, *refs):
    mixed, at = refs[: len(plan)], len(plan)
    out_hbm, staged, sems = refs[-3:]
    rows, model = staged.shape
    stacks = []
    for i, groups in enumerate(plan):
        depth = mixed[i].shape[1] // len(groups)
        for k, pieces in enumerate(groups):
            stacks.append((mixed[i][:, pl.ds(k * depth, depth)], refs[at : at + pieces]))
            at += pieces
    copies = []
    for j in range(0, model, block):
        columns = pl.ds(j, block)
        total = jnp.zeros((rows, block), F32)
        for left, pieces in stacks:
            right = jnp.concatenate([piece[:, columns] for piece in pieces], axis=0)
            total += jnp.dot(left, right, preferred_element_type=F32)
        staged[:, columns] = total.astype(BF16)
        copies.append(pltpu.make_async_copy(staged.at[:, columns], out_hbm.at[:, columns], sems.at[j // block]))
        copies[-1].start()
    for copy in copies:
        copy.wait()


def output(mixed, weights):
    plan = tuple(tuple(len(group) for group in groups) for groups in weights)
    flat = [piece for groups in weights for group in groups for piece in group]
    rows = mixed[0].shape[0]
    model = flat[0].shape[1]
    block = 512 if model % 512 == 0 else model
    return pl.pallas_call(
        functools.partial(output_kernel, plan, block),
        out_shape=jax.ShapeDtypeStruct((rows, model), BF16),
        in_specs=[VMEM_SPEC] * (len(mixed) + len(flat)),
        out_specs=HBM_SPEC,
        scratch_shapes=[pltpu.VMEM((rows, model), BF16), pltpu.SemaphoreType.DMA((model // block,))],
        cost_estimate=cost(2 * rows * model * sum(m.shape[1] for m in mixed)),
        compiler_params=params(8),
        name="output",
    )(*mixed, *flat)


def cut_kernel(w_hbm, first_ref, half_ref, sems):
    quarter, half = first_ref.shape[0], half_ref.shape[0]
    at = lax.axis_index("grp") * quarter
    copies = [
        pltpu.make_async_copy(w_hbm.at[pl.ds(pl.multiple_of(at, quarter), quarter)], first_ref, sems.at[0]),
        pltpu.make_async_copy(w_hbm.at[pl.ds(w_hbm.shape[0] - half, half)], half_ref, sems.at[1]),
    ]
    for copy in copies:
        copy.start()
    for copy in copies:
        copy.wait()


def cut(w_out):
    depth, model = w_out.shape
    shapes = [(depth // 4, model), (depth // 2, model)]
    return pl.pallas_call(
        cut_kernel,
        out_shape=tuple(pltpu.VMEM(shape, BF16) for shape in shapes),
        in_specs=[HBM_SPEC],
        out_specs=(VMEM_SPEC,) * 2,
        scratch_shapes=[pltpu.SemaphoreType.DMA((2,))],
        cost_estimate=cost(1000000),
        compiler_params=params(4),
        name="cut",
    )(in_hbm(w_out))


def tie(x, after):
    return lax.optimization_barrier((x, after))[0]


def layer(tokens, norm_gain, w_query, w_key, w_value, w_out, key_rate):
    shards = lax.axis_size("sp")
    group = lax.axis_size("tp")
    copies = lax.axis_size("grp")
    bits = []
    while 2 << len(bits) <= group:
        bits.append(1 << len(bits))
    bits = bits[::-1]

    def swap(x, bit):
        return lax.ppermute(x, "tp", [(i, i ^ bit) for i in range(group)])

    depth = w_out.shape[0]
    shared = copies == 2 and len(bits) == 2 and depth % (4 * HD) == 0
    if shared:
        first, half = cut(w_out)
        first = swap(first, bits[0])
        half = swap(half, bits[0])
    else:
        weights = [w_out]
        for bit in bits[:-1]:
            weights = weights + [swap(w, bit) for w in weights]

    kv, normed = key_values(tokens, norm_gain, key_rate, w_key, w_value)
    split = shards > 2
    even = shards % 2 == 0
    behind = range(1, shards - 1 if split else shards)
    arrived = []
    for d in behind:
        stop = behind[-1] + 1
        pairs = [(i, (i + 1) % shards) for i in range(shards)] if d == 1 else [(i, i + d) for i in range(stop - d)]
        arrived.append(lax.ppermute(kv, "sp", pairs))
    q, kq = queries(normed, kv, w_query)
    pairs = [(i, i ^ 1) for i in range(shards)] if even else [(shards - 1, shards - 2)]
    if split:
        kq = lax.ppermute(kq, "sp", pairs)
    states = [own_block(q, kv)]
    if shared:
        first = tie(first, states[0][1])
        second = lax.ppermute(first, "grp", [(0, 1), (1, 0)])
        own_core = swap(tie(w_out, states[0][1]), bits[-1])
        first_core = swap(first, bits[-1])
    for i, block in enumerate(arrived):
        last = i == len(arrived) - 1
        if i == 0 and split:
            if last:
                near = more_block(block, states, True, 1)
                far = ahead_blocks(kq, kv, block, q)
                states = near + [far[1].astype(BF16)]
            else:
                states = more_block(block, states, False, 1)
                states = states + [tuple(ahead_blocks(kq, kv, block, q))]
        else:
            states = more_block(block, states, last, 1 if i == 0 else 0)
    if not arrived:
        states = [states[0][1].astype(BF16)]
    near = states[0]

    if split:
        final = lax.axis_index("sp") == shards - 1
        far = states[1]
        pairs = [(i, i ^ 1) for i in range(shards)] if even else [(shards - 2, shards - 1)]
        same = jnp.where(final, lax.ppermute(far, "sp", pairs), 0)
    if split and len(bits) == 2:
        both = [(a * group + i, b * group + (i ^ bits[0])) for a, b in pairs for i in range(group)]
        crossed = lax.ppermute(far, ("sp", "tp"), both)
        near_x = swap(near, bits[0])
        parts = [near + same, near_x + jnp.where(final, crossed, 0)]
    else:
        mixed = near + same if split else near
        for bit in bits[:-1]:
            mixed = jnp.concatenate([mixed, swap(mixed, bit)], axis=1)
        parts = [mixed]
    if shared:
        m = parts[1]
        quarter = depth // 4
        flipped = jnp.concatenate([m[:, quarter : 2 * quarter], m[:, :quarter]], axis=1)
        head = jnp.where(lax.axis_index("grp") == 0, m[:, : 2 * quarter], flipped)
        mixed = jnp.concatenate([parts[0], head, m[:, 2 * quarter :]], axis=1)
        other = swap(mixed, bits[-1])
        second_core = swap(tie(second, near), bits[-1])
        half_core = swap(tie(half, other), bits[-1])
        weights = [[[w_out], [first, second, half]], [[own_core], [first_core, second_core, half_core]]]
    else:
        mixed = parts[0] if len(parts) == 1 else jnp.concatenate(parts, axis=1)
        other = swap(mixed, bits[-1])
        cores = [swap(w_out, bits[-1])] + [swap(tie(w, mixed), bits[-1]) for w in weights[1:]]
        weights = [[[w] for w in weights], [[w] for w in cores]]
    return output([mixed, other], weights)


def solution(mesh):
    return jax.shard_map(
        layer,
        mesh=mesh,
        in_specs=(
            P(("grp", "sp"), None),
            P(),
            P(None, "tp"),
            P(None, "tp"),
            P(None, "tp"),
            P("tp", None),
            P("tp", ("grp", "sp")),
        ),
        out_specs=P(("grp", "sp"), None),
        check_vma=False,
    )
```

```python
import functools

import jax
import jax.numpy as jnp
from jax import lax
from jax.experimental import pallas as pl
from jax.experimental.pallas import tpu as pltpu
from jax.sharding import PartitionSpec as P


HD = 64
EPS = 1e-06
F32 = jnp.float32
BF16 = jnp.bfloat16
VMEM_SPEC = pl.BlockSpec(memory_space=pltpu.VMEM)
HBM_SPEC = pl.BlockSpec(memory_space=pltpu.HBM)


def in_hbm(x):
    return pltpu.with_memory_space_constraint(x, pltpu.HBM)


def params(mib):
    return pltpu.CompilerParams(vmem_limit_bytes=mib << 20)


def cost(flops):
    return pl.CostEstimate(flops=flops, bytes_accessed=1 << 20, transcendentals=0)


def project_kernel(chunks, tok_hbm, gain_hbm, rate_hbm, wk_hbm, wv_hbm, wq_hbm, wo_hbm, kv_ref, q_ref, kq_ref, *refs):
    tok, gain, rate, w, normed, sems, w_sems = refs[-7:]
    rows, model = tok.shape
    width = q_ref.shape[1]
    heads = rate.shape[0]
    depth = model // chunks
    small = []
    for i, (src, dst) in enumerate(((tok_hbm, tok), (gain_hbm, gain), (rate_hbm, rate))):
        small.append(pltpu.make_async_copy(src, dst, sems.at[i]))
        small[-1].start()
    copies = []
    for i, ref in enumerate((wk_hbm, wv_hbm, wq_hbm)):
        for c in range(chunks):
            span = pl.ds(c * depth, depth)
            copies.append(pltpu.make_async_copy(ref.at[span], w.at[i, span], w_sems.at[i, c]))
            copies[-1].start()
    tail = None
    if len(refs) > 7:
        span = pl.ds(wo_hbm.shape[0] - refs[0].shape[0], refs[0].shape[0])
        tail = pltpu.make_async_copy(wo_hbm.at[span], refs[0], sems.at[3])
        tail.start()
    for copy in small:
        copy.wait()
    extra = kv_ref.shape[0] - rows
    for ref in (kv_ref, kq_ref):
        ref[pl.ds(rows, extra), :] = jnp.zeros((extra, 2 * width), BF16)
        ref[pl.ds(rows, heads), pl.ds(0, rows)] = rate[...]
    values = tok[...].astype(F32)
    scale = lax.rsqrt(jnp.mean(values * values, axis=-1, keepdims=True) + EPS)
    normed[...] = (values * scale * gain[...]).astype(BF16)
    for i in range(3):
        total = jnp.zeros((rows, width), F32)
        for c in range(chunks):
            span = pl.ds(c * depth, depth)
            copies[i * chunks + c].wait()
            total += jnp.dot(normed[:, span], w[i, span], preferred_element_type=F32)
        out = total.astype(BF16)
        if i < 2:
            kv_ref[pl.ds(0, rows), pl.ds(i * width, width)] = out
        if i == 0:
            kq_ref[pl.ds(0, rows), pl.ds(0, width)] = out
        if i == 2:
            out = out * jnp.asarray(HD**-0.5, BF16)
            q_ref[...] = out
            kq_ref[pl.ds(0, rows), pl.ds(width, width)] = out
    if tail is not None:
        tail.wait()


def project(tokens, gain, rate, w_key, w_value, w_query, w_out, kept):
    rows, model = tokens.shape
    width = w_query.shape[1]
    chunks = 1
    packed = jax.ShapeDtypeStruct((rows + -(-rate.shape[0] // 8) * 8, 2 * width), BF16)
    operands = (tokens, gain.reshape(1, model), rate, w_key, w_value, w_query, w_out)
    brought = (jax.ShapeDtypeStruct((kept, w_out.shape[1]), BF16),) if kept else ()
    return pl.pallas_call(
        functools.partial(project_kernel, chunks),
        out_shape=(packed, jax.ShapeDtypeStruct((rows, width), BF16), packed) + brought,
        in_specs=[HBM_SPEC] * 7,
        out_specs=(VMEM_SPEC,) * (3 + len(brought)),
        scratch_shapes=[
            pltpu.VMEM((rows, model), BF16),
            pltpu.VMEM((1, model), F32),
            pltpu.VMEM(rate.shape, BF16),
            pltpu.VMEM((3, model, width), BF16),
            pltpu.VMEM((rows, model), BF16),
            pltpu.SemaphoreType.DMA((4,)),
            pltpu.SemaphoreType.DMA((3, chunks)),
        ],
        cost_estimate=cost(6 * rows * model * width),
        compiler_params=params(8),
        name="project",
    )(*(in_hbm(x) for x in operands))


def lanes_of(rows, width):
    return lax.broadcasted_iota(jnp.int32, (rows, width), 1) // HD


def stack_heads(q):
    rows, width = q.shape
    lane = lanes_of(rows, width)
    return jnp.concatenate([jnp.where(lane == h, q, jnp.zeros_like(q)) for h in range(width // HD)], axis=0)


def unstack_heads(spread, rows):
    width = spread.shape[1]
    lane = lanes_of(rows, width)
    total = jnp.zeros((rows, width), F32)
    for h in range(width // HD):
        total = total + jnp.where(lane == h, spread[h * rows : (h + 1) * rows], 0.0)
    return total


def later_matrix(rows):
    start = lax.broadcasted_iota(jnp.int32, (2 * rows, 2 * rows), 0) % rows
    stop = lax.broadcasted_iota(jnp.int32, (2 * rows, 2 * rows), 1)
    return ((start > stop) | (stop >= rows)).astype(F32).astype(BF16)


def logs(stacked, packed, later, diagonal):
    rows = later.shape[0] // 2
    width = stacked.shape[1]
    heads = width // HD
    keys = packed[pl.ds(0, rows), pl.ds(0, width)]
    rate = packed[pl.ds(rows, heads), pl.ds(0, rows)].astype(F32)
    scores = lax.dot_general(stacked, keys, (((1,), (1,)), ((), ())), preferred_element_type=F32)
    scores = jnp.concatenate([scores[h * rows : (h + 1) * rows] + rate[h : h + 1] for h in range(heads)], axis=0)
    softened = jnp.log(1.0 + jnp.exp(-jnp.abs(scores)))
    log_keep = jnp.minimum(scores, 0.0) - softened
    log_remain = -jnp.maximum(scores, 0.0) - softened
    mask = None
    if diagonal:
        q_pos = lax.broadcasted_iota(jnp.int32, scores.shape, 0) % rows
        k_pos = lax.broadcasted_iota(jnp.int32, scores.shape, 1)
        mask = k_pos < q_pos
        log_remain = jnp.where(mask, log_remain, 0.0)
    high = log_remain.astype(BF16)
    low = (log_remain - high.astype(F32)).astype(BF16)
    sums = jnp.dot(jnp.concatenate([high, low], axis=1), later, preferred_element_type=F32)
    return log_keep, sums[:, :rows], sums[:, rows:], mask


def absorb(stacked, packed, later, rest, diagonal=False):
    rows = later.shape[0] // 2
    width = stacked.shape[1]
    log_keep, inside, whole, mask = logs(stacked, packed, later, diagonal)
    exponent = log_keep + inside
    if rest is not None:
        exponent = exponent + rest
        whole = whole + rest
    weight = jnp.exp(exponent)
    if diagonal:
        weight = jnp.where(mask, weight, 0.0)
    values = packed[pl.ds(0, rows), pl.ds(width, width)]
    spread = jnp.dot(weight.astype(BF16), values, preferred_element_type=F32)
    return unstack_heads(spread, rows), whole


def own_kernel(q_ref, kv_ref, acc_ref, rest_ref):
    rows = q_ref.shape[0]
    acc_ref[...], rest_ref[...] = absorb(stack_heads(q_ref[...]), kv_ref, later_matrix(rows), None, True)


def ahead_kernel(kq_ref, own_ref, kv_ref, q_ref, acc_ref, rest_ref):
    rows = acc_ref.shape[0]
    width = kq_ref.shape[1] // 2
    here = lax.axis_index("sp") == lax.axis_size("sp") - 2

    @pl.when(here)
    def _():
        q = kq_ref[pl.ds(0, rows), pl.ds(width, width)]
        q_ref[...] = q
        stacked = stack_heads(q)
        later = later_matrix(rows)
        rest = logs(stacked, kq_ref, later, True)[2] + logs(stacked, own_ref, later, False)[2]
        acc_ref[...], rest_ref[...] = absorb(stacked, kv_ref, later, rest)

    @pl.when(jnp.logical_not(here))
    def _():
        for ref in (q_ref, acc_ref, rest_ref):
            ref[...] = jnp.zeros_like(ref)


def more_kernel(sets, last, distance, split, far, kv_ref, *refs):
    ins, outs = refs[: 3 * sets], refs[3 * sets :]
    per = 1 if last else 2
    rows = ins[0].shape[0]
    here = lax.axis_index("sp")
    final = lax.axis_size("sp") - 1
    for i in range(sets):
        takes = here >= distance
        if split and distance > 1:
            takes = jnp.logical_and(takes, here < final)
        if i == 1 or far:
            takes = here == final - 1
        q_ref, acc_ref, rest_ref = ins[3 * i : 3 * i + 3]
        acc_out = outs[per * i]
        rest_out = None if last else outs[per * i + 1]

        @pl.when(takes)
        def _():
            acc, rest = absorb(stack_heads(q_ref[...]), kv_ref, later_matrix(rows), rest_ref[...])
            acc_out[...] = (acc + acc_ref[...]).astype(acc_out.dtype)
            if not last:
                rest_out[...] = rest

        @pl.when(jnp.logical_not(takes))
        def _():
            acc_out[...] = acc_ref[...].astype(acc_out.dtype)
            if not last:
                rest_out[...] = rest_ref[...]


def state_shapes(q, last=False):
    rows, width = q.shape
    if last:
        return (jax.ShapeDtypeStruct((rows, width), BF16),)
    return (
        jax.ShapeDtypeStruct((rows, width), F32),
        jax.ShapeDtypeStruct((width // HD * rows, rows), F32),
    )


def local_call(kernel, flops, out_shape, *operands):
    return pl.pallas_call(
        kernel,
        out_shape=out_shape,
        in_specs=[VMEM_SPEC] * len(operands),
        out_specs=(VMEM_SPEC,) * len(out_shape),
        cost_estimate=cost(flops),
        compiler_params=params(12),
    )(*operands)


def own_block(q, kv):
    return (q, *local_call(own_kernel, 600000000, state_shapes(q), q, kv))


def ahead_blocks(kq, own, kv, q):
    shapes = (jax.ShapeDtypeStruct(q.shape, BF16), *state_shapes(q))
    return local_call(ahead_kernel, 1200000000, shapes, kq, own, kv)


def more_block(kv, states, last, distance, split, far=False):
    q = states[0][0]
    sets = len(states)
    flat = [x for state in states for x in state]
    out = local_call(
        functools.partial(more_kernel, sets, last, distance, split, far), 600000000 * sets, state_shapes(q, last) * sets, kv, *flat
    )
    if last:
        return list(out)
    return [(states[i][0], out[2 * i], out[2 * i + 1]) for i in range(sets)]


def partial_kernel(plan, block, *refs):
    out_ref = refs[-1]
    rows, model = out_ref.shape
    at = 0
    stacks = []
    for has_far, pieces, flips in plan:
        left = refs[at][...]
        at += 1
        if has_far:
            final = lax.axis_index("sp") == lax.axis_size("sp") - 1
            left = left.astype(F32) + jnp.where(final, refs[at][...].astype(F32), 0.0)
            at += 1
        stacks.append((left.astype(BF16), refs[at : at + pieces], flips))
        at += pieces
    for j in range(0, model, block):
        columns = pl.ds(j, block)
        total = jnp.zeros((rows, block), F32)
        for left, pieces, flips in stacks:
            right = [piece[:, columns] for piece in pieces]
            if flips:
                keep = lax.axis_index("grp") == 0
                right[:2] = [jnp.where(keep, right[0], right[1]), jnp.where(keep, right[1], right[0])]
            right = jnp.concatenate(right, axis=0)
            total += jnp.dot(left, right, preferred_element_type=F32)
        out_ref[:, columns] = total.astype(BF16)


def partial_output(stacks):
    plan, flat = [], []
    for near, far, pieces, flips in stacks:
        plan.append((far is not None, len(pieces), flips))
        flat += [near] + ([] if far is None else [far]) + list(pieces)
    rows, depth = stacks[0][0].shape
    model = stacks[0][2][0].shape[1]
    block = 512 if model % 512 == 0 else model
    return pl.pallas_call(
        functools.partial(partial_kernel, tuple(plan), block),
        out_shape=jax.ShapeDtypeStruct((rows, model), BF16),
        in_specs=[VMEM_SPEC] * len(flat),
        out_specs=VMEM_SPEC,
        cost_estimate=cost(2 * rows * model * depth * len(stacks)),
        compiler_params=params(4),
        name="partial",
    )(*flat)


def cut_kernel(w_hbm, first_ref, sem):
    first = first_ref.shape[0]
    at = pl.multiple_of(lax.axis_index("grp") * first, first)
    copy = pltpu.make_async_copy(w_hbm.at[pl.ds(at, first)], first_ref, sem)
    copy.start()
    copy.wait()


def cut(w_out, share):
    return pl.pallas_call(
        cut_kernel,
        out_shape=pltpu.VMEM((share, w_out.shape[1]), BF16),
        in_specs=[HBM_SPEC],
        out_specs=VMEM_SPEC,
        scratch_shapes=[pltpu.SemaphoreType.DMA],
        cost_estimate=cost(1000000),
        compiler_params=params(4),
        name="cut",
    )(in_hbm(w_out))


def tie(x, after):
    return lax.optimization_barrier((x, after))[0]


def layer(tokens, norm_gain, w_query, w_key, w_value, w_out, key_rate):
    shards = lax.axis_size("sp")
    group = lax.axis_size("tp")
    copies = lax.axis_size("grp")
    bits = []
    while 2 << len(bits) <= group:
        bits.append(1 << len(bits))
    bits = bits[::-1]

    def swap(x, bit):
        return lax.ppermute(x, "tp", [(i, i ^ bit) for i in range(group)])

    depth = w_out.shape[0]
    shared = copies == 2 and len(bits) == 2 and depth == 256
    weights = [[w_out]]
    if shared:
        share = depth * 5 // 16
        first = cut(w_out, share)
        first = swap(first, bits[0])
    else:
        for bit in bits[:-1]:
            weights = weights + [[swap(w[0], bit)] for w in weights]

    kept = depth - 2 * share if shared else 0
    kv, q, kq, *half = project(tokens, norm_gain, key_rate, w_key, w_value, w_query, w_out, kept)
    if shared:
        half = swap(half[0], bits[0])
    split = shards > 2
    even = shards % 2 == 0
    behind = range(1, shards - 1 if split else shards)
    arrived = []
    for d in behind:
        stop = behind[-1] + 1
        pairs = [(i, (i + 1) % shards) for i in range(shards)] if d == 1 else [(i, i + d) for i in range(stop - d)]
        arrived.append(lax.ppermute(kv, "sp", pairs))
    if split:
        kq = lax.ppermute(kq, "sp", [(shards - 1, shards - 2)])
    states = [own_block(q, kv)]
    if shared:
        first = tie(first, states[0][1])
        second = lax.ppermute(first, "grp", [(0, 1), (1, 0)])
        weights = weights + [[first, second, half]]
    for i, block in enumerate(arrived):
        last = i == len(arrived) - 1
        if i == 0 and split:
            if last:
                near = more_block(block, states, True, 1, split)
                far = ahead_blocks(kq, kv, block, q)
                states = near + [far[1].astype(BF16)]
            else:
                states = more_block(block, states, False, 1, split)
                kq = tie(kq, states[0][1])
                states = states + [tuple(ahead_blocks(kq, kv, block, q))]
        elif last and len(states) == 2:
            behind_part = more_block(block, states[1:], True, i + 1, split, True)
            states = more_block(block, states[:1], True, i + 1, split) + behind_part
        else:
            states = more_block(block, states, last, i + 1, split)
    if not arrived:
        states = [states[0][1].astype(BF16)]
    near = [states[0]]
    far = [None]

    if split:
        pairs = [(i, i ^ 1) for i in range(shards)] if even else [(shards - 2, shards - 1)]
        far = [lax.ppermute(states[1], "sp", pairs)]
        if len(bits) == 2:
            both = [(a * group + i, b * group + (i ^ bits[0])) for a, b in pairs for i in range(group)]
            far.append(lax.ppermute(states[1], ("sp", "tp"), both))
        else:
            near = [near[0] + jnp.where(lax.axis_index("sp") == shards - 1, far[0], 0)]
            far = [None]
    for bit in bits[:-1]:
        near = near + [swap(x, bit) for x in near]
    far = far + [None] * (len(near) - len(far))
    flips = [shared and i == 1 for i in range(len(near))]
    part = partial_output(list(zip(near, far, weights, flips)))
    if not bits:
        return part
    other = swap(part, bits[-1])
    return (part.astype(F32) + other.astype(F32)).astype(BF16)


def solution(mesh):
    return jax.shard_map(
        layer,
        mesh=mesh,
        in_specs=(
            P(("grp", "sp"), None),
            P(),
            P(None, "tp"),
            P(None, "tp"),
            P(None, "tp"),
            P("tp", None),
            P("tp", ("grp", "sp")),
        ),
        out_specs=P(("grp", "sp"), None),
        check_vma=False,
    )
```

```python
import functools

import jax
import jax.numpy as jnp
from jax import lax
from jax.experimental import pallas as pl
from jax.experimental.pallas import tpu as pltpu
from jax.sharding import PartitionSpec as P


LOG2E = 1.4426950408889634
HD = 64
EPS = 1e-06
F32 = jnp.float32
BF16 = jnp.bfloat16
VMEM_SPEC = pl.BlockSpec(memory_space=pltpu.VMEM)
HBM_SPEC = pl.BlockSpec(memory_space=pltpu.HBM)


def in_hbm(x):
    return pltpu.with_memory_space_constraint(x, pltpu.HBM)


def params(mib):
    return pltpu.CompilerParams(vmem_limit_bytes=mib << 20)


def cost(flops):
    return pl.CostEstimate(flops=flops, bytes_accessed=1 << 20, transcendentals=0)


def project_kernel(chunks, tok_hbm, gain_hbm, rate_hbm, wk_hbm, wv_hbm, wq_hbm, wo_hbm, kv_ref, q_ref, *refs):
    tok, gain, rate, w, normed, sems, w_sems = refs[-7:]
    rows, model = tok.shape
    width = q_ref.shape[1]
    heads = rate.shape[0]
    depth = model // chunks
    small = []
    for i, (src, dst) in enumerate(((tok_hbm, tok), (gain_hbm, gain), (rate_hbm, rate))):
        small.append(pltpu.make_async_copy(src, dst, sems.at[i]))
        small[-1].start()
    copies = []
    for i, ref in enumerate((wk_hbm, wv_hbm, wq_hbm)):
        for c in range(chunks):
            span = pl.ds(c * depth, depth)
            copies.append(pltpu.make_async_copy(ref.at[span], w.at[i, span], w_sems.at[i, c]))
            copies[-1].start()
    tail = None
    if len(refs) > 7:
        span = pl.ds(wo_hbm.shape[0] - refs[0].shape[0], refs[0].shape[0])
        tail = pltpu.make_async_copy(wo_hbm.at[span], refs[0], sems.at[3])
        tail.start()
    for copy in small:
        copy.wait()
    extra = kv_ref.shape[0] - rows
    kv_ref[pl.ds(rows, extra), :] = jnp.zeros((extra, 2 * width), BF16)
    kv_ref[pl.ds(rows, heads), pl.ds(0, rows)] = rate[...]
    values = tok[...].astype(F32)
    scale = lax.rsqrt(jnp.mean(values * values, axis=-1, keepdims=True) + EPS)
    normed[...] = (values * scale * gain[...]).astype(BF16)
    for i in range(3):
        total = jnp.zeros((rows, width), F32)
        for c in range(chunks):
            span = pl.ds(c * depth, depth)
            copies[i * chunks + c].wait()
            total += jnp.dot(normed[:, span], w[i, span], preferred_element_type=F32)
        out = total.astype(BF16)
        if i < 2:
            kv_ref[pl.ds(0, rows), pl.ds(i * width, width)] = out
        if i == 2:
            q_ref[...] = out * jnp.asarray(HD**-0.5, BF16)
    if tail is not None:
        tail.wait()


def project(tokens, gain, rate, w_key, w_value, w_query, w_out, kept):
    rows, model = tokens.shape
    width = w_query.shape[1]
    chunks = 1
    packed = jax.ShapeDtypeStruct((rows + -(-rate.shape[0] // 8) * 8, 2 * width), BF16)
    operands = (tokens, gain.reshape(1, model), rate, w_key, w_value, w_query, w_out)
    brought = (jax.ShapeDtypeStruct((kept, w_out.shape[1]), BF16),) if kept else ()
    return pl.pallas_call(
        functools.partial(project_kernel, chunks),
        out_shape=(packed, jax.ShapeDtypeStruct((rows, width), BF16)) + brought,
        in_specs=[HBM_SPEC] * 7,
        out_specs=(VMEM_SPEC,) * (2 + len(brought)),
        scratch_shapes=[
            pltpu.VMEM((rows, model), BF16),
            pltpu.VMEM((1, model), F32),
            pltpu.VMEM(rate.shape, BF16),
            pltpu.VMEM((3, model, width), BF16),
            pltpu.VMEM((rows, model), BF16),
            pltpu.SemaphoreType.DMA((4,)),
            pltpu.SemaphoreType.DMA((3, chunks)),
        ],
        cost_estimate=cost(6 * rows * model * width),
        compiler_params=params(8),
        name="project",
    )(*(in_hbm(x) for x in operands))


def lanes_of(rows, width):
    return lax.broadcasted_iota(jnp.int32, (rows, width), 1) // HD


def stack_heads(q):
    rows, width = q.shape
    lane = lanes_of(rows, width)
    return jnp.concatenate([jnp.where(lane == h, q, jnp.zeros_like(q)) for h in range(width // HD)], axis=0)


def unstack_heads(spread, rows):
    width = spread.shape[1]
    lane = lanes_of(rows, width)
    total = jnp.zeros((rows, width), F32)
    for h in range(width // HD):
        total = total + jnp.where(lane == h, spread[h * rows : (h + 1) * rows], 0.0)
    return total


def later_matrix(rows):
    start = lax.broadcasted_iota(jnp.int32, (2 * rows, 2 * rows), 0) % rows
    stop = lax.broadcasted_iota(jnp.int32, (2 * rows, 2 * rows), 1)
    return ((start > stop) | (stop >= rows)).astype(F32).astype(BF16)


def logs(stacked, packed, later, diagonal):
    rows = later.shape[0] // 2
    width = stacked.shape[1]
    heads = width // HD
    keys = packed[pl.ds(0, rows), pl.ds(0, width)]
    rate = packed[pl.ds(rows, heads), pl.ds(0, rows)].astype(F32)
    scores = lax.dot_general(stacked, keys, (((1,), (1,)), ((), ())), preferred_element_type=F32)
    scores = jnp.concatenate([scores[h * rows : (h + 1) * rows] + rate[h : h + 1] for h in range(heads)], axis=0)
    scores = scores * LOG2E
    softened = jnp.log2(1.0 + jnp.exp2(-jnp.abs(scores)))
    log_keep = jnp.minimum(scores, 0.0) - softened
    log_remain = -jnp.maximum(scores, 0.0) - softened
    mask = None
    if diagonal:
        q_pos = lax.broadcasted_iota(jnp.int32, scores.shape, 0) % rows
        k_pos = lax.broadcasted_iota(jnp.int32, scores.shape, 1)
        mask = k_pos < q_pos
        log_remain = jnp.where(mask, log_remain, 0.0)
    high = log_remain.astype(BF16)
    low = (log_remain - high.astype(F32)).astype(BF16)
    sums = jnp.dot(jnp.concatenate([high, low], axis=1), later, preferred_element_type=F32)
    return log_keep, sums[:, :rows], sums[:, rows:], mask


def absorb(stacked, packed, later, rest, diagonal=False):
    rows = later.shape[0] // 2
    width = stacked.shape[1]
    log_keep, inside, whole, mask = logs(stacked, packed, later, diagonal)
    exponent = log_keep + inside
    if rest is not None:
        exponent = exponent + rest
        whole = whole + rest
    weight = jnp.exp2(exponent)
    if diagonal:
        weight = jnp.where(mask, weight, 0.0)
    values = packed[pl.ds(0, rows), pl.ds(width, width)]
    spread = jnp.dot(weight.astype(BF16), values, preferred_element_type=F32)
    return unstack_heads(spread, rows), whole


def own_kernel(q_ref, kv_ref, acc_ref, rest_ref):
    rows = q_ref.shape[0]
    acc_ref[...], rest_ref[...] = absorb(stack_heads(q_ref[...]), kv_ref, later_matrix(rows), None, True)


def ahead_kernel(q_ref, kv_ref, acc_ref, rest_ref):
    rows = q_ref.shape[0]
    here = lax.axis_index("sp") == lax.axis_size("sp") - 2

    @pl.when(here)
    def _():
        acc_ref[...], rest_ref[...] = absorb(stack_heads(q_ref[...]), kv_ref, later_matrix(rows), None)

    @pl.when(jnp.logical_not(here))
    def _():
        for ref in (acc_ref, rest_ref):
            ref[...] = jnp.zeros_like(ref)


def far_factor(rest, rows, heads):
    lines = [jnp.transpose(rest[h * rows : (h + 1) * rows])[:1] for h in range(heads)]
    return jnp.exp2(jnp.concatenate(lines, axis=0)).astype(BF16)


def add_far(near_ref, far_ref, out_ref):
    rows, width = far_ref.shape
    heads = width // HD
    final = lax.axis_index("sp") == lax.axis_size("sp") - 1

    @pl.when(jnp.logical_not(final))
    def _():
        out_ref[...] = near_ref[pl.ds(0, rows), :]

    @pl.when(final)
    def _():
        factor = near_ref[pl.ds(rows, heads), pl.ds(0, rows)]
        lane = lax.broadcasted_iota(jnp.int32, (heads, width), 1) // HD
        pick = (lane == lax.broadcasted_iota(jnp.int32, (heads, width), 0)).astype(F32).astype(BF16)
        wide = lax.dot_general(factor, pick, (((0,), (0,)), ((), ())), preferred_element_type=F32)
        total = near_ref[pl.ds(0, rows), :].astype(F32) + far_ref[...].astype(F32) * wide
        out_ref[...] = total.astype(BF16)


def more_kernel(sets, last, distance, split, far, kv_ref, *refs):
    ins, outs = refs[: 3 * sets], refs[3 * sets :]
    per = 1 if last else 2
    rows = ins[0].shape[0]
    here = lax.axis_index("sp")
    final = lax.axis_size("sp") - 1
    for i in range(sets):
        takes = here >= distance
        if split and distance > 1:
            takes = jnp.logical_and(takes, here < final)
        if i == 1 or far:
            takes = here == final - 1
        q_ref, acc_ref, rest_ref = ins[3 * i : 3 * i + 3]
        acc_out = outs[per * i]
        rest_out = None if last else outs[per * i + 1]
        heads = acc_ref.shape[1] // HD
        tails = last and split and i == 0 and not far

        @pl.when(takes)
        def _():
            acc, rest = absorb(stack_heads(q_ref[...]), kv_ref, later_matrix(rows), rest_ref[...])
            acc_out[pl.ds(0, rows), :] = (acc + acc_ref[...]).astype(acc_out.dtype)
            if tails:
                acc_out[pl.ds(rows, heads), pl.ds(0, rows)] = far_factor(rest, rows, heads)
            if not last:
                rest_out[...] = rest

        @pl.when(jnp.logical_not(takes))
        def _():
            acc_out[pl.ds(0, rows), :] = acc_ref[...].astype(acc_out.dtype)
            if tails:
                acc_out[pl.ds(rows, heads), pl.ds(0, rows)] = far_factor(rest_ref[...], rows, heads)
            if not last:
                rest_out[...] = rest_ref[...]


def state_shapes(q, last=False):
    rows, width = q.shape
    if last:
        return (jax.ShapeDtypeStruct((rows, width), BF16),)
    return (
        jax.ShapeDtypeStruct((rows, width), F32),
        jax.ShapeDtypeStruct((width // HD * rows, rows), F32),
    )


def local_call(kernel, flops, out_shape, *operands):
    return pl.pallas_call(
        kernel,
        out_shape=out_shape,
        in_specs=[VMEM_SPEC] * len(operands),
        out_specs=(VMEM_SPEC,) * len(out_shape),
        cost_estimate=cost(flops),
        compiler_params=params(12),
    )(*operands)


def own_block(q, kv):
    return (q, *local_call(own_kernel, 600000000, state_shapes(q), q, kv))


def ahead_blocks(q, kv):
    return (q, *local_call(ahead_kernel, 600000000, state_shapes(q), q, kv))


def more_block(kv, states, last, distance, split, far=False):
    q = states[0][0]
    sets = len(states)
    flat = [x for state in states for x in state]
    shapes = state_shapes(q, last) * sets
    if last and split and not far:
        rows, width = q.shape
        shapes = (jax.ShapeDtypeStruct((rows + -(-(width // HD) // 8) * 8, width), BF16), *shapes[1:])
    kernel = functools.partial(more_kernel, sets, last, distance, split, far)
    out = local_call(kernel, 600000000 * sets, shapes, kv, *flat)
    if last:
        return list(out)
    return [(states[i][0], out[2 * i], out[2 * i + 1]) for i in range(sets)]


def merge(near, far):
    return local_call(add_far, 1000000, (jax.ShapeDtypeStruct(far.shape, BF16),), near, far)[0]


def partial_kernel(plan, block, *refs):
    out_ref, merged = refs[-2:]
    rows, model = out_ref.shape
    at = 0
    stacks = []
    for has_far, pieces, flips in plan:
        if has_far:
            add_far(refs[at], refs[at + 1], merged)
            left = merged[...]
            at += 2
        else:
            left = refs[at][...]
            at += 1
        stacks.append((left, refs[at : at + pieces], flips))
        at += pieces
    for j in range(0, model, block):
        columns = pl.ds(j, block)
        total = jnp.zeros((rows, block), F32)
        for left, pieces, flips in stacks:
            right = [piece[:, columns] for piece in pieces]
            if flips:
                keep = lax.axis_index("grp") == 0
                right[:2] = [jnp.where(keep, right[0], right[1]), jnp.where(keep, right[1], right[0])]
            right = jnp.concatenate(right, axis=0)
            total += jnp.dot(left, right, preferred_element_type=F32)
        out_ref[:, columns] = total.astype(BF16)


def partial_output(stacks):
    plan, flat = [], []
    for near, far, pieces, flips in stacks:
        plan.append((far is not None, len(pieces), flips))
        flat += [near] + ([] if far is None else [far]) + list(pieces)
    rows, depth = (stacks[0][0] if stacks[0][1] is None else stacks[0][1]).shape
    model = stacks[0][2][0].shape[1]
    block = 512 if model % 512 == 0 else model
    return pl.pallas_call(
        functools.partial(partial_kernel, tuple(plan), block),
        out_shape=jax.ShapeDtypeStruct((rows, model), BF16),
        in_specs=[VMEM_SPEC] * len(flat),
        out_specs=VMEM_SPEC,
        scratch_shapes=[pltpu.VMEM((rows, depth), BF16)],
        cost_estimate=cost(2 * rows * model * depth * len(stacks)),
        compiler_params=params(4),
        name="partial",
    )(*flat)


def finish_kernel(span, mine_ref, theirs_ref, out_hbm, staged, sems):
    copies = []
    for i in range(staged.shape[0] // span):
        run = pl.ds(i * span, span)
        staged[run, :] = (mine_ref[run, :].astype(F32) + theirs_ref[run, :].astype(F32)).astype(BF16)
        copies.append(pltpu.make_async_copy(staged.at[run], out_hbm.at[run], sems.at[i]))
        copies[-1].start()
    for copy in copies:
        copy.wait()


def finish(mine, theirs):
    rows, model = mine.shape
    span = 32 if rows % 32 == 0 else rows
    return pl.pallas_call(
        functools.partial(finish_kernel, span),
        out_shape=jax.ShapeDtypeStruct((rows, model), BF16),
        in_specs=[VMEM_SPEC] * 2,
        out_specs=HBM_SPEC,
        scratch_shapes=[pltpu.VMEM((rows, model), BF16), pltpu.SemaphoreType.DMA((rows // span,))],
        cost_estimate=cost(1000000),
        compiler_params=params(4),
        name="finish",
    )(mine, theirs)


def cut_kernel(w_hbm, first_ref, sem):
    first = first_ref.shape[0]
    at = pl.multiple_of(lax.axis_index("grp") * first, first)
    copy = pltpu.make_async_copy(w_hbm.at[pl.ds(at, first)], first_ref, sem)
    copy.start()
    copy.wait()


def cut(w_out, share):
    return pl.pallas_call(
        cut_kernel,
        out_shape=pltpu.VMEM((share, w_out.shape[1]), BF16),
        in_specs=[HBM_SPEC],
        out_specs=VMEM_SPEC,
        scratch_shapes=[pltpu.SemaphoreType.DMA],
        cost_estimate=cost(1000000),
        compiler_params=params(4),
        name="cut",
    )(in_hbm(w_out))


def tie(x, after):
    return lax.optimization_barrier((x, after))[0]


def layer(tokens, norm_gain, w_query, w_key, w_value, w_out, key_rate):
    shards = lax.axis_size("sp")
    group = lax.axis_size("tp")
    copies = lax.axis_size("grp")
    bits = []
    while 2 << len(bits) <= group:
        bits.append(1 << len(bits))
    bits = bits[::-1]

    def swap(x, bit):
        return lax.ppermute(x, "tp", [(i, i ^ bit) for i in range(group)])

    depth = w_out.shape[0]
    shared = copies == 2 and len(bits) == 2 and depth == 256
    weights = [[w_out]]
    if shared:
        share = depth * 5 // 16
        first = cut(w_out, share)
        first = swap(first, bits[0])
    else:
        for bit in bits[:-1]:
            weights = weights + [[swap(w[0], bit)] for w in weights]

    kept = depth - 2 * share if shared else 0
    kv, q, *half = project(tokens, norm_gain, key_rate, w_key, w_value, w_query, w_out, kept)
    if shared:
        half = swap(half[0], bits[0])
    split = shards > 2 and w_query.shape[1] >= tokens.shape[0]
    even = shards % 2 == 0
    behind = range(1, shards - 1 if split else shards)
    arrived = []
    for d in behind:
        stop = behind[-1] + 1
        pairs = [(i, (i + 1) % shards) for i in range(shards)] if d == 1 else [(i, i + d) for i in range(stop - d)]
        arrived.append(lax.ppermute(kv, "sp", pairs))
    if split:
        last_q = lax.ppermute(q, "sp", [(shards - 1, shards - 2)])
    states = [own_block(q, kv)]
    if shared:
        first = tie(first, states[0][1])
        second = lax.ppermute(first, "grp", [(0, 1), (1, 0)])
        weights = weights + [[first, second, half]]
    for i, block in enumerate(arrived):
        last = i == len(arrived) - 1
        if i == 0 and split:
            if last:
                near = more_block(block, states, True, 1, split)
                far = ahead_blocks(last_q, block)
                states = near + [far[1].astype(BF16)]
            else:
                states = more_block(block, states, False, 1, split)
                last_q = tie(last_q, states[0][1])
                states = states + [ahead_blocks(last_q, block)]
        elif last and len(states) == 2:
            behind_part = more_block(block, states[1:], True, i + 1, split, True)
            states = more_block(block, states[:1], True, i + 1, split) + behind_part
        else:
            states = more_block(block, states, last, i + 1, split)
    if not arrived:
        states = [states[0][1].astype(BF16)]
    near = [states[0]]
    far = [None]

    if split:
        pairs = [(i, i ^ 1) for i in range(shards)] if even else [(shards - 2, shards - 1)]
        far = [lax.ppermute(states[1], "sp", pairs)]
        if len(bits) == 2:
            both = [(a * group + i, b * group + (i ^ bits[0])) for a, b in pairs for i in range(group)]
            far.append(lax.ppermute(states[1], ("sp", "tp"), both))
        else:
            near = [merge(near[0], far[0])]
            far = [None]
    for bit in bits[:-1]:
        near = near + [swap(x, bit) for x in near]
    if len(far) == 2:
        near[1], far[1] = merge(near[1], far[1]), None
    far = far + [None] * (len(near) - len(far))
    flips = [shared and i == 1 for i in range(len(near))]
    part = partial_output(list(zip(near, far, weights, flips)))
    if not bits:
        return part
    other = swap(part, bits[-1])
    return finish(part, other)


def solution(mesh):
    return jax.shard_map(
        layer,
        mesh=mesh,
        in_specs=(
            P(("grp", "sp"), None),
            P(),
            P(None, "tp"),
            P(None, "tp"),
            P(None, "tp"),
            P("tp", None),
            P("tp", ("grp", "sp")),
        ),
        out_specs=P(("grp", "sp"), None),
        check_vma=False,
    )
```

```python
import functools

import jax
import jax.numpy as jnp
from jax import lax
from jax.experimental import pallas as pl
from jax.experimental.pallas import tpu as pltpu
from jax.sharding import PartitionSpec as P


LATE_BLOCK = 256
LOG2E = 1.4426950408889634
HD = 64
EPS = 1e-06
F32 = jnp.float32
BF16 = jnp.bfloat16
VMEM_SPEC = pl.BlockSpec(memory_space=pltpu.VMEM)
HBM_SPEC = pl.BlockSpec(memory_space=pltpu.HBM)


def in_hbm(x):
    return pltpu.with_memory_space_constraint(x, pltpu.HBM)


def params(mib):
    return pltpu.CompilerParams(vmem_limit_bytes=mib << 20)


def cost(flops):
    return pl.CostEstimate(flops=flops, bytes_accessed=1 << 20, transcendentals=0)


def project_kernel(chunks, tok_hbm, gain_hbm, rate_hbm, wk_hbm, wv_hbm, wq_hbm, wo_hbm, kv_ref, q_ref, *refs):
    tok, gain, rate, w, normed, sems, w_sems = refs[-7:]
    rows, model = tok.shape
    width = q_ref.shape[1]
    heads = rate.shape[0]
    depth = model // chunks
    small = []
    for i, (src, dst) in enumerate(((tok_hbm, tok), (gain_hbm, gain), (rate_hbm, rate))):
        small.append(pltpu.make_async_copy(src, dst, sems.at[i]))
        small[-1].start()
    copies = []
    for i, ref in enumerate((wk_hbm, wv_hbm, wq_hbm)):
        for c in range(chunks):
            span = pl.ds(c * depth, depth)
            copies.append(pltpu.make_async_copy(ref.at[span], w.at[i, span], w_sems.at[i, c]))
            copies[-1].start()
    tail = None
    if len(refs) > 7:
        span = pl.ds(wo_hbm.shape[0] - refs[0].shape[0], refs[0].shape[0])
        tail = pltpu.make_async_copy(wo_hbm.at[span], refs[0], sems.at[3])
        tail.start()
    for copy in small:
        copy.wait()
    extra = kv_ref.shape[0] - rows
    kv_ref[pl.ds(rows, extra), :] = jnp.zeros((extra, 2 * width), BF16)
    kv_ref[pl.ds(rows, heads), pl.ds(0, rows)] = rate[...]
    values = tok[...].astype(F32)
    scale = lax.rsqrt(jnp.mean(values * values, axis=-1, keepdims=True) + EPS)
    normed[...] = (values * scale * gain[...]).astype(BF16)
    for i in range(3):
        total = jnp.zeros((rows, width), F32)
        for c in range(chunks):
            span = pl.ds(c * depth, depth)
            copies[i * chunks + c].wait()
            total += jnp.dot(normed[:, span], w[i, span], preferred_element_type=F32)
        out = total.astype(BF16)
        if i < 2:
            kv_ref[pl.ds(0, rows), pl.ds(i * width, width)] = out
        if i == 2:
            q_ref[...] = out * jnp.asarray(HD**-0.5, BF16)
    if tail is not None:
        tail.wait()


def project(tokens, gain, rate, w_key, w_value, w_query, w_out, kept):
    rows, model = tokens.shape
    width = w_query.shape[1]
    chunks = 1
    packed = jax.ShapeDtypeStruct((rows + -(-rate.shape[0] // 8) * 8, 2 * width), BF16)
    operands = (tokens, gain.reshape(1, model), rate, w_key, w_value, w_query, w_out)
    brought = (jax.ShapeDtypeStruct((kept, w_out.shape[1]), BF16),) if kept else ()
    return pl.pallas_call(
        functools.partial(project_kernel, chunks),
        out_shape=(packed, jax.ShapeDtypeStruct((rows, width), BF16)) + brought,
        in_specs=[HBM_SPEC] * 7,
        out_specs=(VMEM_SPEC,) * (2 + len(brought)),
        scratch_shapes=[
            pltpu.VMEM((rows, model), BF16),
            pltpu.VMEM((1, model), F32),
            pltpu.VMEM(rate.shape, BF16),
            pltpu.VMEM((3, model, width), BF16),
            pltpu.VMEM((rows, model), BF16),
            pltpu.SemaphoreType.DMA((4,)),
            pltpu.SemaphoreType.DMA((3, chunks)),
        ],
        cost_estimate=cost(6 * rows * model * width),
        compiler_params=params(8),
        name="project",
    )(*(in_hbm(x) for x in operands))


def lanes_of(rows, width):
    return lax.broadcasted_iota(jnp.int32, (rows, width), 1) // HD


def stack_heads(q):
    rows, width = q.shape
    lane = lanes_of(rows, width)
    return jnp.concatenate([jnp.where(lane == h, q, jnp.zeros_like(q)) for h in range(width // HD)], axis=0)


def unstack_heads(spread, rows):
    width = spread.shape[1]
    lane = lanes_of(rows, width)
    total = jnp.zeros((rows, width), F32)
    for h in range(width // HD):
        total = total + jnp.where(lane == h, spread[h * rows : (h + 1) * rows], 0.0)
    return total


def later_matrix(rows):
    start = lax.broadcasted_iota(jnp.int32, (2 * rows, 2 * rows), 0) % rows
    stop = lax.broadcasted_iota(jnp.int32, (2 * rows, 2 * rows), 1)
    return ((start > stop) | (stop >= rows)).astype(F32).astype(BF16)


def logs(stacked, packed, later, diagonal):
    rows = later.shape[0] // 2
    width = stacked.shape[1]
    heads = width // HD
    keys = packed[pl.ds(0, rows), pl.ds(0, width)]
    rate = packed[pl.ds(rows, heads), pl.ds(0, rows)].astype(F32)
    scores = lax.dot_general(stacked, keys, (((1,), (1,)), ((), ())), preferred_element_type=F32)
    scores = jnp.concatenate([scores[h * rows : (h + 1) * rows] + rate[h : h + 1] for h in range(heads)], axis=0)
    scores = scores * LOG2E
    softened = jnp.log2(1.0 + jnp.exp2(-jnp.abs(scores)))
    log_keep = jnp.minimum(scores, 0.0) - softened
    log_remain = -jnp.maximum(scores, 0.0) - softened
    mask = None
    if diagonal:
        q_pos = lax.broadcasted_iota(jnp.int32, scores.shape, 0) % rows
        k_pos = lax.broadcasted_iota(jnp.int32, scores.shape, 1)
        mask = k_pos < q_pos
        log_remain = jnp.where(mask, log_remain, 0.0)
    high = log_remain.astype(BF16)
    low = (log_remain - high.astype(F32)).astype(BF16)
    sums = jnp.dot(jnp.concatenate([high, low], axis=1), later, preferred_element_type=F32)
    return log_keep, sums[:, :rows], sums[:, rows:], mask


def absorb(stacked, packed, later, rest, diagonal=False):
    rows = later.shape[0] // 2
    width = stacked.shape[1]
    log_keep, inside, whole, mask = logs(stacked, packed, later, diagonal)
    exponent = log_keep + inside
    if rest is not None:
        exponent = exponent + rest
        whole = whole + rest
    weight = jnp.exp2(exponent)
    if diagonal:
        weight = jnp.where(mask, weight, 0.0)
    values = packed[pl.ds(0, rows), pl.ds(width, width)]
    spread = jnp.dot(weight.astype(BF16), values, preferred_element_type=F32)
    return unstack_heads(spread, rows), whole


def own_kernel(q_ref, kv_ref, acc_ref, rest_ref):
    rows = q_ref.shape[0]
    acc_ref[...], rest_ref[...] = absorb(stack_heads(q_ref[...]), kv_ref, later_matrix(rows), None, True)


def ahead_kernel(q_ref, kv_ref, acc_ref, rest_ref):
    rows = q_ref.shape[0]
    here = lax.axis_index("sp") == lax.axis_size("sp") - 2

    @pl.when(here)
    def _():
        acc_ref[...], rest_ref[...] = absorb(stack_heads(q_ref[...]), kv_ref, later_matrix(rows), None)

    @pl.when(jnp.logical_not(here))
    def _():
        for ref in (acc_ref, rest_ref):
            ref[...] = jnp.zeros_like(ref)


def far_factor(rest, rows, heads):
    lines = [jnp.transpose(rest[h * rows : (h + 1) * rows])[:1] for h in range(heads)]
    return jnp.exp2(jnp.concatenate(lines, axis=0)).astype(BF16)


def merge_both_kernel(near_ref, far_ref, near_x_ref, far_x_ref, out_ref):
    width = far_ref.shape[1]
    add_far(near_ref, far_ref, out_ref.at[:, pl.ds(0, width)])
    add_far(near_x_ref, far_x_ref, out_ref.at[:, pl.ds(width, width)])


def merge_both(near, far, near_x, far_x):
    rows, width = far.shape
    shape = (jax.ShapeDtypeStruct((rows, 2 * width), BF16),)
    return local_call(merge_both_kernel, 1000000, shape, near, far, near_x, far_x)[0]


def add_far(near_ref, far_ref, out_ref):
    rows, width = far_ref.shape
    heads = width // HD
    final = lax.axis_index("sp") == lax.axis_size("sp") - 1

    @pl.when(jnp.logical_not(final))
    def _():
        out_ref[...] = near_ref[pl.ds(0, rows), :]

    @pl.when(final)
    def _():
        factor = near_ref[pl.ds(rows, heads), pl.ds(0, rows)]
        lane = lax.broadcasted_iota(jnp.int32, (heads, width), 1) // HD
        pick = (lane == lax.broadcasted_iota(jnp.int32, (heads, width), 0)).astype(F32).astype(BF16)
        wide = lax.dot_general(factor, pick, (((0,), (0,)), ((), ())), preferred_element_type=F32)
        total = near_ref[pl.ds(0, rows), :].astype(F32) + far_ref[...].astype(F32) * wide
        out_ref[...] = total.astype(BF16)


def more_kernel(sets, last, distance, split, far, kv_ref, *refs):
    ins, outs = refs[: 3 * sets], refs[3 * sets :]
    per = 1 if last else 2
    rows = ins[0].shape[0]
    here = lax.axis_index("sp")
    final = lax.axis_size("sp") - 1
    for i in range(sets):
        takes = here >= distance
        if split and distance > 1:
            takes = jnp.logical_and(takes, here < final)
        if i == 1 or far:
            takes = here == final - 1
        q_ref, acc_ref, rest_ref = ins[3 * i : 3 * i + 3]
        acc_out = outs[per * i]
        rest_out = None if last else outs[per * i + 1]
        heads = acc_ref.shape[1] // HD
        tails = last and split and i == 0 and not far

        @pl.when(takes)
        def _():
            acc, rest = absorb(stack_heads(q_ref[...]), kv_ref, later_matrix(rows), rest_ref[...])
            acc_out[pl.ds(0, rows), :] = (acc + acc_ref[...]).astype(acc_out.dtype)
            if tails:
                acc_out[pl.ds(rows, heads), pl.ds(0, rows)] = far_factor(rest, rows, heads)
            if not last:
                rest_out[...] = rest

        @pl.when(jnp.logical_not(takes))
        def _():
            acc_out[pl.ds(0, rows), :] = acc_ref[...].astype(acc_out.dtype)
            if tails:
                acc_out[pl.ds(rows, heads), pl.ds(0, rows)] = far_factor(rest_ref[...], rows, heads)
            if not last:
                rest_out[...] = rest_ref[...]


def state_shapes(q, last=False):
    rows, width = q.shape
    if last:
        return (jax.ShapeDtypeStruct((rows, width), BF16),)
    return (
        jax.ShapeDtypeStruct((rows, width), F32),
        jax.ShapeDtypeStruct((width // HD * rows, rows), F32),
    )


def local_call(kernel, flops, out_shape, *operands):
    return pl.pallas_call(
        kernel,
        out_shape=out_shape,
        in_specs=[VMEM_SPEC] * len(operands),
        out_specs=(VMEM_SPEC,) * len(out_shape),
        cost_estimate=cost(flops),
        compiler_params=params(12),
    )(*operands)


def own_block(q, kv):
    return (q, *local_call(own_kernel, 600000000, state_shapes(q), q, kv))


def ahead_blocks(q, kv):
    return (q, *local_call(ahead_kernel, 600000000, state_shapes(q), q, kv))


def more_block(kv, states, last, distance, split, far=False):
    q = states[0][0]
    sets = len(states)
    flat = [x for state in states for x in state]
    shapes = state_shapes(q, last) * sets
    if last and split and not far:
        rows, width = q.shape
        shapes = (jax.ShapeDtypeStruct((rows + -(-(width // HD) // 8) * 8, width), BF16), *shapes[1:])
    kernel = functools.partial(more_kernel, sets, last, distance, split, far)
    out = local_call(kernel, 600000000 * sets, shapes, kv, *flat)
    if last:
        return list(out)
    return [(states[i][0], out[2 * i], out[2 * i + 1]) for i in range(sets)]


def merge(near, far):
    return local_call(add_far, 1000000, (jax.ShapeDtypeStruct(far.shape, BF16),), near, far)[0]


def partial_kernel(plan, block, *refs):
    out_ref, merged = refs[-2:]
    rows, model = out_ref.shape
    at = 0
    stacks = []
    for has_far, pieces, flips in plan:
        if has_far:
            add_far(refs[at], refs[at + 1], merged)
            left = merged[...]
            at += 2
        else:
            left = refs[at][...]
            at += 1
        stacks.append((left, refs[at : at + pieces], flips))
        at += pieces
    for j in range(0, model, block):
        columns = pl.ds(j, block)
        total = jnp.zeros((rows, block), F32)
        for left, pieces, flips in stacks:
            right = [piece[:, columns] for piece in pieces]
            if flips:
                keep = lax.axis_index("grp") == 0
                right[:2] = [jnp.where(keep, right[0], right[1]), jnp.where(keep, right[1], right[0])]
            right = jnp.concatenate(right, axis=0)
            total += jnp.dot(left, right, preferred_element_type=F32)
        out_ref[:, columns] = total.astype(BF16)


def partial_output(stacks):
    plan, flat = [], []
    for near, far, pieces, flips in stacks:
        plan.append((far is not None, len(pieces), flips))
        flat += [near] + ([] if far is None else [far]) + list(pieces)
    rows, depth = (stacks[0][0] if stacks[0][1] is None else stacks[0][1]).shape
    model = stacks[0][2][0].shape[1]
    block = 512 if model % 512 == 0 else model
    return pl.pallas_call(
        functools.partial(partial_kernel, tuple(plan), block),
        out_shape=jax.ShapeDtypeStruct((rows, model), BF16),
        in_specs=[VMEM_SPEC] * len(flat),
        out_specs=VMEM_SPEC,
        scratch_shapes=[pltpu.VMEM((rows, depth), BF16)],
        cost_estimate=cost(2 * rows * model * depth * len(stacks)),
        compiler_params=params(4),
        name="partial",
    )(*flat)


def stacks_of(plan, refs):
    depth = refs[0].shape[1] // len(plan)
    at, stacks = 1, []
    for i, (pieces, flips) in enumerate(plan):
        stacks.append((refs[0][:, pl.ds(i * depth, depth)], refs[at : at + pieces], flips))
        at += pieces
    return stacks


def columns_of(stacks, columns, total):
    for left, pieces, flips in stacks:
        right = [piece[:, columns] for piece in pieces]
        for k in range(0, flips, 2):
            keep = lax.axis_index("grp") == 0
            one, two = right[k : k + 2]
            right[k : k + 2] = [jnp.where(keep, one, two), jnp.where(keep, two, one)]
        total += jnp.dot(left, jnp.concatenate(right, axis=0), preferred_element_type=F32)
    return total


def early_kernel(plan, block, *refs):
    out_ref = refs[-1]
    rows, model = out_ref.shape
    stacks = stacks_of(plan, refs[:-1])
    for j in range(0, model, block):
        columns = pl.ds(j, block)
        out_ref[:, columns] = columns_of(stacks, columns, jnp.zeros((rows, block), F32))


def late_kernel(plan, block, early_ref, *refs):
    out_hbm, staged, sems = refs[-3:]
    model = staged.shape[1]
    stacks = stacks_of(plan, refs[:-3])
    copies = []
    for j in range(0, model, block):
        columns = pl.ds(j, block)
        staged[:, columns] = columns_of(stacks, columns, early_ref[:, columns]).astype(BF16)
        copies.append(pltpu.make_async_copy(staged.at[:, columns], out_hbm.at[:, columns], sems.at[j // block]))
        copies[-1].start()
    for copy in copies:
        copy.wait()


def summed_output(results, groups, early):
    plan = tuple((len(pieces), flips) for pieces, flips in groups)
    flat = [results] + [x for pieces, _ in groups for x in pieces]
    rows = results.shape[0]
    model = flat[1].shape[1]
    block = LATE_BLOCK if model % LATE_BLOCK == 0 else model
    if early is None:
        kernel, operands, dtype, scratch = early_kernel, flat, F32, []
    else:
        kernel, operands, dtype = late_kernel, [early] + flat, BF16
        scratch = [pltpu.VMEM((rows, model), BF16), pltpu.SemaphoreType.DMA((model // block,))]
    return pl.pallas_call(
        functools.partial(kernel, plan, block),
        out_shape=jax.ShapeDtypeStruct((rows, model), dtype),
        in_specs=[VMEM_SPEC] * len(operands),
        out_specs=VMEM_SPEC if early is None else HBM_SPEC,
        scratch_shapes=scratch,
        cost_estimate=cost(2 * rows * model * results.shape[1]),
        compiler_params=params(6),
    )(*operands)


def finish_kernel(span, mine_ref, theirs_ref, out_hbm, staged, sems):
    copies = []
    for i in range(staged.shape[0] // span):
        run = pl.ds(i * span, span)
        staged[run, :] = (mine_ref[run, :].astype(F32) + theirs_ref[run, :].astype(F32)).astype(BF16)
        copies.append(pltpu.make_async_copy(staged.at[run], out_hbm.at[run], sems.at[i]))
        copies[-1].start()
    for copy in copies:
        copy.wait()


def finish(mine, theirs):
    rows, model = mine.shape
    span = 32 if rows % 32 == 0 else rows
    return pl.pallas_call(
        functools.partial(finish_kernel, span),
        out_shape=jax.ShapeDtypeStruct((rows, model), BF16),
        in_specs=[VMEM_SPEC] * 2,
        out_specs=HBM_SPEC,
        scratch_shapes=[pltpu.VMEM((rows, model), BF16), pltpu.SemaphoreType.DMA((rows // span,))],
        cost_estimate=cost(1000000),
        compiler_params=params(4),
        name="finish",
    )(mine, theirs)


def cut_kernel(w_hbm, first_ref, sem):
    first = first_ref.shape[0]
    at = pl.multiple_of(lax.axis_index("grp") * first, first)
    copy = pltpu.make_async_copy(w_hbm.at[pl.ds(at, first)], first_ref, sem)
    copy.start()
    copy.wait()


def cut(w_out, share):
    return pl.pallas_call(
        cut_kernel,
        out_shape=pltpu.VMEM((share, w_out.shape[1]), BF16),
        in_specs=[HBM_SPEC],
        out_specs=VMEM_SPEC,
        scratch_shapes=[pltpu.SemaphoreType.DMA],
        cost_estimate=cost(1000000),
        compiler_params=params(4),
        name="cut",
    )(in_hbm(w_out))


def tie(x, after):
    return lax.optimization_barrier((x, after))[0]


def layer(tokens, norm_gain, w_query, w_key, w_value, w_out, key_rate):
    shards = lax.axis_size("sp")
    group = lax.axis_size("tp")
    copies = lax.axis_size("grp")
    bits = []
    while 2 << len(bits) <= group:
        bits.append(1 << len(bits))
    bits = bits[::-1]

    def swap(x, bit):
        return lax.ppermute(x, "tp", [(i, i ^ bit) for i in range(group)])

    depth = w_out.shape[0]
    shared = copies == 2 and len(bits) == 2 and depth == 256
    weights = [[w_out]]
    if shared:
        share = depth * 5 // 16
        first = cut(w_out, share)
        first = swap(first, bits[0])
    else:
        for bit in bits[:-1]:
            weights = weights + [[swap(w[0], bit)] for w in weights]

    kept = depth - 2 * share if shared else 0
    kv, q, *half = project(tokens, norm_gain, key_rate, w_key, w_value, w_query, w_out, kept)
    if shared:
        half = swap(half[0], bits[0])
    split = shards > 2 and w_query.shape[1] >= tokens.shape[0]
    even = shards % 2 == 0
    behind = range(1, shards - 1 if split else shards)
    arrived = []
    for d in behind:
        stop = behind[-1] + 1
        pairs = [(i, (i + 1) % shards) for i in range(shards)] if d == 1 else [(i, i + d) for i in range(stop - d)]
        arrived.append(lax.ppermute(kv, "sp", pairs))
    if split:
        last_q = lax.ppermute(q, "sp", [(shards - 1, shards - 2)])
    states = [own_block(q, kv)]
    if shared:
        first = tie(first, states[0][1])
        second = lax.ppermute(first, "grp", [(0, 1), (1, 0)])
        weights = weights + [[first, second, half]]
        if split:
            own_core = swap(tie(w_out, states[0][1]), bits[-1])
            first_core = swap(tie(first, states[0][1]), bits[-1])
    for i, block in enumerate(arrived):
        last = i == len(arrived) - 1
        if i == 0 and split:
            if last:
                near = more_block(block, states, True, 1, split)
                far = ahead_blocks(last_q, block)
                states = near + [far[1].astype(BF16)]
            else:
                states = more_block(block, states, False, 1, split)
                last_q = tie(last_q, states[0][1])
                states = states + [ahead_blocks(last_q, block)]
        elif last and len(states) == 2:
            behind_part = more_block(block, states[1:], True, i + 1, split, True)
            states = more_block(block, states[:1], True, i + 1, split) + behind_part
        else:
            states = more_block(block, states, last, i + 1, split)
    if not arrived:
        states = [states[0][1].astype(BF16)]
    near = [states[0]]
    far = [None]

    if split:
        pairs = [(i, i ^ 1) for i in range(shards)] if even else [(shards - 2, shards - 1)]
        far = [lax.ppermute(states[1], "sp", pairs)]
        if len(bits) == 2:
            both = [(a * group + i, b * group + (i ^ bits[0])) for a, b in pairs for i in range(group)]
            far.append(lax.ppermute(states[1], ("sp", "tp"), both))
        else:
            near = [merge(near[0], far[0])]
            far = [None]
    for bit in bits[:-1]:
        near = near + [swap(x, bit) for x in near]
    if len(far) == 2 and shared:
        half_core = swap(tie(half, states[0]), bits[-1])
        second_core = swap(tie(second, states[0]), bits[-1])
        both = merge_both(near[0], far[0], near[1], far[1])
        both_core = swap(both, bits[-1])
        early = summed_output(both, [([w_out], 0), (weights[1], 2)], None)
        cores = [([own_core], 0), ([first_core, second_core, half_core], 2)]
        return summed_output(both_core, cores, early)
    if len(far) == 2:
        near[1], far[1] = merge(near[1], far[1]), None
    far = far + [None] * (len(near) - len(far))
    flips = [shared and i == 1 for i in range(len(near))]
    part = partial_output(list(zip(near, far, weights, flips)))
    if not bits:
        return part
    other = swap(part, bits[-1])
    return finish(part, other)


def solution(mesh):
    return jax.shard_map(
        layer,
        mesh=mesh,
        in_specs=(
            P(("grp", "sp"), None),
            P(),
            P(None, "tp"),
            P(None, "tp"),
            P(None, "tp"),
            P("tp", None),
            P("tp", ("grp", "sp")),
        ),
        out_specs=P(("grp", "sp"), None),
        check_vma=False,
    )
```

```python
import functools

import jax
import jax.numpy as jnp
from jax import lax
from jax.experimental import pallas as pl
from jax.experimental.pallas import tpu as pltpu
from jax.sharding import PartitionSpec as P


LATE_BLOCK = 512
LOG2E = 1.4426950408889634
HD = 64
EPS = 1e-06
F32 = jnp.float32
BF16 = jnp.bfloat16
VMEM_SPEC = pl.BlockSpec(memory_space=pltpu.VMEM)
HBM_SPEC = pl.BlockSpec(memory_space=pltpu.HBM)


def in_hbm(x):
    return pltpu.with_memory_space_constraint(x, pltpu.HBM)


def params(mib):
    return pltpu.CompilerParams(vmem_limit_bytes=mib << 20)


def cost(flops):
    return pl.CostEstimate(flops=flops, bytes_accessed=1 << 20, transcendentals=0)


def project_kernel(chunks, tok_hbm, gain_hbm, rate_hbm, wk_hbm, wv_hbm, wq_hbm, wo_hbm, kv_ref, q_ref, *refs):
    tok, gain, rate, w, normed, sems, w_sems = refs[-7:]
    rows, model = tok.shape
    width = q_ref.shape[1]
    heads = rate.shape[0]
    depth = model // chunks
    small = []
    for i, (src, dst) in enumerate(((tok_hbm, tok), (gain_hbm, gain), (rate_hbm, rate))):
        small.append(pltpu.make_async_copy(src, dst, sems.at[i]))
        small[-1].start()
    copies = []
    for i, ref in enumerate((wk_hbm, wv_hbm, wq_hbm)):
        for c in range(chunks):
            span = pl.ds(c * depth, depth)
            copies.append(pltpu.make_async_copy(ref.at[span], w.at[i, span], w_sems.at[i, c]))
            copies[-1].start()
    tail = None
    if len(refs) > 7:
        span = pl.ds(wo_hbm.shape[0] - refs[0].shape[0], refs[0].shape[0])
        tail = pltpu.make_async_copy(wo_hbm.at[span], refs[0], sems.at[3])
        tail.start()
    for copy in small:
        copy.wait()
    extra = kv_ref.shape[0] - rows
    kv_ref[pl.ds(rows, extra), :] = jnp.zeros((extra, 2 * width), BF16)
    kv_ref[pl.ds(rows, heads), pl.ds(0, rows)] = rate[...]
    values = tok[...].astype(F32)
    scale = lax.rsqrt(jnp.mean(values * values, axis=-1, keepdims=True) + EPS)
    normed[...] = (values * scale * gain[...]).astype(BF16)
    for i in range(3):
        total = jnp.zeros((rows, width), F32)
        for c in range(chunks):
            span = pl.ds(c * depth, depth)
            copies[i * chunks + c].wait()
            total += jnp.dot(normed[:, span], w[i, span], preferred_element_type=F32)
        out = total.astype(BF16)
        if i < 2:
            kv_ref[pl.ds(0, rows), pl.ds(i * width, width)] = out
        if i == 2:
            q_ref[...] = out * jnp.asarray(HD**-0.5, BF16)
    if tail is not None:
        tail.wait()


def project(tokens, gain, rate, w_key, w_value, w_query, w_out, kept):
    rows, model = tokens.shape
    width = w_query.shape[1]
    chunks = 1
    packed = jax.ShapeDtypeStruct((rows + -(-rate.shape[0] // 8) * 8, 2 * width), BF16)
    operands = (tokens, gain.reshape(1, model), rate, w_key, w_value, w_query, w_out)
    brought = (jax.ShapeDtypeStruct((kept, w_out.shape[1]), BF16),) if kept else ()
    return pl.pallas_call(
        functools.partial(project_kernel, chunks),
        out_shape=(packed, jax.ShapeDtypeStruct((rows, width), BF16)) + brought,
        in_specs=[HBM_SPEC] * 7,
        out_specs=(VMEM_SPEC,) * (2 + len(brought)),
        scratch_shapes=[
            pltpu.VMEM((rows, model), BF16),
            pltpu.VMEM((1, model), F32),
            pltpu.VMEM(rate.shape, BF16),
            pltpu.VMEM((3, model, width), BF16),
            pltpu.VMEM((rows, model), BF16),
            pltpu.SemaphoreType.DMA((4,)),
            pltpu.SemaphoreType.DMA((3, chunks)),
        ],
        cost_estimate=cost(6 * rows * model * width),
        compiler_params=params(8),
        name="project",
    )(*(in_hbm(x) for x in operands))


def lanes_of(rows, width):
    return lax.broadcasted_iota(jnp.int32, (rows, width), 1) // HD


def stack_heads(q):
    rows, width = q.shape
    lane = lanes_of(rows, width)
    return jnp.concatenate([jnp.where(lane == h, q, jnp.zeros_like(q)) for h in range(width // HD)], axis=0)


def unstack_heads(spread, rows):
    width = spread.shape[1]
    lane = lanes_of(rows, width)
    total = jnp.zeros((rows, width), F32)
    for h in range(width // HD):
        total = total + jnp.where(lane == h, spread[h * rows : (h + 1) * rows], 0.0)
    return total


def later_matrix(rows):
    start = lax.broadcasted_iota(jnp.int32, (2 * rows, 2 * rows), 0) % rows
    stop = lax.broadcasted_iota(jnp.int32, (2 * rows, 2 * rows), 1)
    return ((start > stop) | (stop >= rows)).astype(F32).astype(BF16)


def logs(stacked, packed, later, diagonal):
    rows = later.shape[0] // 2
    width = stacked.shape[1]
    heads = width // HD
    keys = packed[pl.ds(0, rows), pl.ds(0, width)]
    rate = packed[pl.ds(rows, heads), pl.ds(0, rows)].astype(F32)
    scores = lax.dot_general(stacked, keys, (((1,), (1,)), ((), ())), preferred_element_type=F32)
    scores = jnp.concatenate([scores[h * rows : (h + 1) * rows] + rate[h : h + 1] for h in range(heads)], axis=0)
    scores = scores * LOG2E
    softened = jnp.log2(1.0 + jnp.exp2(-jnp.abs(scores)))
    log_keep = jnp.minimum(scores, 0.0) - softened
    log_remain = -jnp.maximum(scores, 0.0) - softened
    mask = None
    if diagonal:
        q_pos = lax.broadcasted_iota(jnp.int32, scores.shape, 0) % rows
        k_pos = lax.broadcasted_iota(jnp.int32, scores.shape, 1)
        mask = k_pos < q_pos
        log_remain = jnp.where(mask, log_remain, 0.0)
    high = log_remain.astype(BF16)
    low = (log_remain - high.astype(F32)).astype(BF16)
    sums = jnp.dot(jnp.concatenate([high, low], axis=1), later, preferred_element_type=F32)
    return log_keep, sums[:, :rows], sums[:, rows:], mask


def absorb(stacked, packed, later, rest, diagonal=False):
    rows = later.shape[0] // 2
    width = stacked.shape[1]
    log_keep, inside, whole, mask = logs(stacked, packed, later, diagonal)
    exponent = log_keep + inside
    if rest is not None:
        exponent = exponent + rest
        whole = whole + rest
    weight = jnp.exp2(exponent)
    if diagonal:
        weight = jnp.where(mask, weight, 0.0)
    values = packed[pl.ds(0, rows), pl.ds(width, width)]
    spread = jnp.dot(weight.astype(BF16), values, preferred_element_type=F32)
    return unstack_heads(spread, rows), whole


def own_kernel(q_ref, kv_ref, acc_ref, rest_ref):
    rows = q_ref.shape[0]
    acc_ref[...], rest_ref[...] = absorb(stack_heads(q_ref[...]), kv_ref, later_matrix(rows), None, True)


def ahead_kernel(q_ref, kv_ref, acc_ref, rest_ref):
    rows = q_ref.shape[0]
    here = lax.axis_index("sp") == lax.axis_size("sp") - 2

    @pl.when(here)
    def _():
        acc_ref[...], rest_ref[...] = absorb(stack_heads(q_ref[...]), kv_ref, later_matrix(rows), None)

    @pl.when(jnp.logical_not(here))
    def _():
        for ref in (acc_ref, rest_ref):
            ref[...] = jnp.zeros_like(ref)


def far_factor(rest, rows, heads):
    lines = [jnp.transpose(rest[h * rows : (h + 1) * rows])[:1] for h in range(heads)]
    return jnp.exp2(jnp.concatenate(lines, axis=0)).astype(BF16)


def merge_both_kernel(near_ref, far_ref, near_x_ref, far_x_ref, out_ref):
    width = far_ref.shape[1]
    add_far(near_ref, far_ref, out_ref.at[:, pl.ds(0, width)])
    add_far(near_x_ref, far_x_ref, out_ref.at[:, pl.ds(width, width)])


def merge_both(near, far, near_x, far_x):
    rows, width = far.shape
    shape = (jax.ShapeDtypeStruct((rows, 2 * width), BF16),)
    return local_call(merge_both_kernel, 1000000, shape, near, far, near_x, far_x)[0]


def add_far(near_ref, far_ref, out_ref):
    rows, width = far_ref.shape
    heads = width // HD
    final = lax.axis_index("sp") == lax.axis_size("sp") - 1

    @pl.when(jnp.logical_not(final))
    def _():
        out_ref[...] = near_ref[pl.ds(0, rows), :]

    @pl.when(final)
    def _():
        factor = near_ref[pl.ds(rows, heads), pl.ds(0, rows)]
        lane = lax.broadcasted_iota(jnp.int32, (heads, width), 1) // HD
        pick = (lane == lax.broadcasted_iota(jnp.int32, (heads, width), 0)).astype(F32).astype(BF16)
        wide = lax.dot_general(factor, pick, (((0,), (0,)), ((), ())), preferred_element_type=F32)
        total = near_ref[pl.ds(0, rows), :].astype(F32) + far_ref[...].astype(F32) * wide
        out_ref[...] = total.astype(BF16)


def more_kernel(sets, last, distance, split, far, kv_ref, *refs):
    ins, outs = refs[: 3 * sets], refs[3 * sets :]
    per = 1 if last else 2
    rows = ins[0].shape[0]
    here = lax.axis_index("sp")
    final = lax.axis_size("sp") - 1
    for i in range(sets):
        takes = here >= distance
        if split and distance > 1:
            takes = jnp.logical_and(takes, here < final)
        if i == 1 or far:
            takes = here == final - 1
        q_ref, acc_ref, rest_ref = ins[3 * i : 3 * i + 3]
        acc_out = outs[per * i]
        rest_out = None if last else outs[per * i + 1]
        heads = acc_ref.shape[1] // HD
        tails = last and split and i == 0 and not far

        @pl.when(takes)
        def _():
            acc, rest = absorb(stack_heads(q_ref[...]), kv_ref, later_matrix(rows), rest_ref[...])
            acc_out[pl.ds(0, rows), :] = (acc + acc_ref[...]).astype(acc_out.dtype)
            if tails:
                acc_out[pl.ds(rows, heads), pl.ds(0, rows)] = far_factor(rest, rows, heads)
            if not last:
                rest_out[...] = rest

        @pl.when(jnp.logical_not(takes))
        def _():
            acc_out[pl.ds(0, rows), :] = acc_ref[...].astype(acc_out.dtype)
            if tails:
                acc_out[pl.ds(rows, heads), pl.ds(0, rows)] = far_factor(rest_ref[...], rows, heads)
            if not last:
                rest_out[...] = rest_ref[...]


def state_shapes(q, last=False):
    rows, width = q.shape
    if last:
        return (jax.ShapeDtypeStruct((rows, width), BF16),)
    return (
        jax.ShapeDtypeStruct((rows, width), F32),
        jax.ShapeDtypeStruct((width // HD * rows, rows), F32),
    )


def local_call(kernel, flops, out_shape, *operands):
    return pl.pallas_call(
        kernel,
        out_shape=out_shape,
        in_specs=[VMEM_SPEC] * len(operands),
        out_specs=(VMEM_SPEC,) * len(out_shape),
        cost_estimate=cost(flops),
        compiler_params=params(12),
    )(*operands)


def own_block(q, kv):
    return (q, *local_call(own_kernel, 600000000, state_shapes(q), q, kv))


def ahead_blocks(q, kv):
    return (q, *local_call(ahead_kernel, 600000000, state_shapes(q), q, kv))


def more_block(kv, states, last, distance, split, far=False):
    q = states[0][0]
    sets = len(states)
    flat = [x for state in states for x in state]
    shapes = state_shapes(q, last) * sets
    if last and split and not far:
        rows, width = q.shape
        shapes = (jax.ShapeDtypeStruct((rows + -(-(width // HD) // 8) * 8, width), BF16), *shapes[1:])
    kernel = functools.partial(more_kernel, sets, last, distance, split, far)
    out = local_call(kernel, 600000000 * sets, shapes, kv, *flat)
    if last:
        return list(out)
    return [(states[i][0], out[2 * i], out[2 * i + 1]) for i in range(sets)]


def merge(near, far):
    return local_call(add_far, 1000000, (jax.ShapeDtypeStruct(far.shape, BF16),), near, far)[0]


def partial_kernel(plan, block, *refs):
    out_ref, merged = refs[-2:]
    rows, model = out_ref.shape
    at = 0
    stacks = []
    for has_far, pieces, flips in plan:
        if has_far:
            add_far(refs[at], refs[at + 1], merged)
            left = merged[...]
            at += 2
        else:
            left = refs[at][...]
            at += 1
        stacks.append((left, refs[at : at + pieces], flips))
        at += pieces
    for j in range(0, model, block):
        columns = pl.ds(j, block)
        total = jnp.zeros((rows, block), F32)
        for left, pieces, flips in stacks:
            right = [piece[:, columns] for piece in pieces]
            if flips:
                keep = lax.axis_index("grp") == 0
                right[:2] = [jnp.where(keep, right[0], right[1]), jnp.where(keep, right[1], right[0])]
            right = jnp.concatenate(right, axis=0)
            total += jnp.dot(left, right, preferred_element_type=F32)
        out_ref[:, columns] = total.astype(BF16)


def partial_output(stacks):
    plan, flat = [], []
    for near, far, pieces, flips in stacks:
        plan.append((far is not None, len(pieces), flips))
        flat += [near] + ([] if far is None else [far]) + list(pieces)
    rows, depth = (stacks[0][0] if stacks[0][1] is None else stacks[0][1]).shape
    model = stacks[0][2][0].shape[1]
    block = 512 if model % 512 == 0 else model
    return pl.pallas_call(
        functools.partial(partial_kernel, tuple(plan), block),
        out_shape=jax.ShapeDtypeStruct((rows, model), BF16),
        in_specs=[VMEM_SPEC] * len(flat),
        out_specs=VMEM_SPEC,
        scratch_shapes=[pltpu.VMEM((rows, depth), BF16)],
        cost_estimate=cost(2 * rows * model * depth * len(stacks)),
        compiler_params=params(4),
        name="partial",
    )(*flat)


def stacks_of(plan, refs):
    depth = refs[0].shape[1] // len(plan)
    at, stacks = 1, []
    for i, (pieces, flips) in enumerate(plan):
        stacks.append((refs[0][:, pl.ds(i * depth, depth)], refs[at : at + pieces], flips))
        at += pieces
    return stacks


def columns_of(stacks, columns, total):
    lefts, rights = [], []
    for left, pieces, flips in stacks:
        right = [piece[:, columns] for piece in pieces]
        for k in range(0, flips, 2):
            keep = lax.axis_index("grp") == 0
            one, two = right[k : k + 2]
            right[k : k + 2] = [jnp.where(keep, one, two), jnp.where(keep, two, one)]
        lefts.append(left)
        rights += right
    left, right = jnp.concatenate(lefts, axis=1), jnp.concatenate(rights, axis=0)
    product = jnp.dot(left, right, preferred_element_type=F32)
    return product if total is None else product + total


def early_kernel(plan, block, *refs):
    out_ref = refs[-1]
    _, model = out_ref.shape
    stacks = stacks_of(plan, refs[:-1])
    for j in range(0, model, block):
        columns = pl.ds(j, block)
        out_ref[:, columns] = columns_of(stacks, columns, None)


def late_kernel(plan, block, early_ref, *refs):
    out_hbm, staged, sems = refs[-3:]
    model = staged.shape[1]
    stacks = stacks_of(plan, refs[:-3])
    copies = []
    for j in range(0, model, block):
        columns = pl.ds(j, block)
        staged[:, columns] = columns_of(stacks, columns, early_ref[:, columns]).astype(BF16)
        copies.append(pltpu.make_async_copy(staged.at[:, columns], out_hbm.at[:, columns], sems.at[j // block]))
        copies[-1].start()
    for copy in copies:
        copy.wait()


def summed_output(results, groups, early):
    plan = tuple((len(pieces), flips) for pieces, flips in groups)
    flat = [results] + [x for pieces, _ in groups for x in pieces]
    rows = results.shape[0]
    model = flat[1].shape[1]
    block = LATE_BLOCK if model % LATE_BLOCK == 0 else model
    if early is None:
        kernel, operands, dtype, scratch = early_kernel, flat, F32, []
    else:
        kernel, operands, dtype = late_kernel, [early] + flat, BF16
        scratch = [pltpu.VMEM((rows, model), BF16), pltpu.SemaphoreType.DMA((model // block,))]
    return pl.pallas_call(
        functools.partial(kernel, plan, block),
        out_shape=jax.ShapeDtypeStruct((rows, model), dtype),
        in_specs=[VMEM_SPEC] * len(operands),
        out_specs=VMEM_SPEC if early is None else HBM_SPEC,
        scratch_shapes=scratch,
        cost_estimate=cost(2 * rows * model * results.shape[1]),
        compiler_params=params(6),
    )(*operands)


def finish_kernel(span, mine_ref, theirs_ref, out_hbm, staged, sems):
    copies = []
    for i in range(staged.shape[0] // span):
        run = pl.ds(i * span, span)
        staged[run, :] = (mine_ref[run, :].astype(F32) + theirs_ref[run, :].astype(F32)).astype(BF16)
        copies.append(pltpu.make_async_copy(staged.at[run], out_hbm.at[run], sems.at[i]))
        copies[-1].start()
    for copy in copies:
        copy.wait()


def finish(mine, theirs):
    rows, model = mine.shape
    span = 32 if rows % 32 == 0 else rows
    return pl.pallas_call(
        functools.partial(finish_kernel, span),
        out_shape=jax.ShapeDtypeStruct((rows, model), BF16),
        in_specs=[VMEM_SPEC] * 2,
        out_specs=HBM_SPEC,
        scratch_shapes=[pltpu.VMEM((rows, model), BF16), pltpu.SemaphoreType.DMA((rows // span,))],
        cost_estimate=cost(1000000),
        compiler_params=params(4),
        name="finish",
    )(mine, theirs)


def tie(x, after):
    return lax.optimization_barrier((x, after))[0]


def layer(tokens, norm_gain, w_query, w_key, w_value, w_out, key_rate):
    shards = lax.axis_size("sp")
    group = lax.axis_size("tp")
    copies = lax.axis_size("grp")
    bits = []
    while 2 << len(bits) <= group:
        bits.append(1 << len(bits))
    bits = bits[::-1]

    def swap(x, bit):
        return lax.ppermute(x, "tp", [(i, i ^ bit) for i in range(group)])

    depth = w_out.shape[0]
    shared = copies == 2 and len(bits) == 2 and depth == 256
    weights = [[w_out]]
    if shared:
        share = depth * 5 // 16
        first = lax.dynamic_slice_in_dim(w_out, lax.axis_index("grp") * share, share, 0)
        first = swap(first, bits[0])
    else:
        for bit in bits[:-1]:
            weights = weights + [[swap(w[0], bit)] for w in weights]

    kept = depth - 2 * share if shared else 0
    kv, q, *half = project(tokens, norm_gain, key_rate, w_key, w_value, w_query, w_out, kept)
    if shared:
        half = swap(half[0], bits[0])
    split = shards > 2 and w_query.shape[1] >= tokens.shape[0]
    even = shards % 2 == 0
    behind = range(1, shards - 1 if split else shards)
    arrived = []
    for d in behind:
        stop = behind[-1] + 1
        pairs = [(i, (i + 1) % shards) for i in range(shards)] if d == 1 else [(i, i + d) for i in range(stop - d)]
        arrived.append(lax.ppermute(kv, "sp", pairs))
    if split:
        last_q = lax.ppermute(q, "sp", [(shards - 1, shards - 2)])
    states = [own_block(q, kv)]
    if shared:
        first = tie(first, states[0][1])
        second = lax.ppermute(first, "grp", [(0, 1), (1, 0)])
        weights = weights + [[first, second, half]]
        if split:
            own_core = swap(tie(w_out, states[0][1]), bits[-1])
            first_core = swap(tie(first, states[0][1]), bits[-1])
    for i, block in enumerate(arrived):
        last = i == len(arrived) - 1
        if i == 0 and split:
            if last:
                near = more_block(block, states, True, 1, split)
                far = ahead_blocks(last_q, block)
                states = near + [far[1].astype(BF16)]
            else:
                states = more_block(block, states, False, 1, split)
                last_q = tie(last_q, states[0][1])
                states = states + [ahead_blocks(last_q, block)]
        elif last and len(states) == 2:
            behind_part = more_block(block, states[1:], True, i + 1, split, True)
            states = more_block(block, states[:1], True, i + 1, split) + behind_part
        else:
            states = more_block(block, states, last, i + 1, split)
    if not arrived:
        states = [states[0][1].astype(BF16)]
    near = [states[0]]
    far = [None]

    if split:
        pairs = [(i, i ^ 1) for i in range(shards)] if even else [(shards - 2, shards - 1)]
        far = [lax.ppermute(states[1], "sp", pairs)]
        if len(bits) == 2:
            both = [(a * group + i, b * group + (i ^ bits[0])) for a, b in pairs for i in range(group)]
            far.append(lax.ppermute(states[1], ("sp", "tp"), both))
        else:
            near = [merge(near[0], far[0])]
            far = [None]
    for bit in bits[:-1]:
        near = near + [swap(x, bit) for x in near]
    if len(far) == 2 and shared:
        half_core = swap(tie(half, states[0]), bits[-1])
        second_core = swap(tie(second, states[0]), bits[-1])
        both = merge_both(near[0], far[0], near[1], far[1])
        both_core = swap(both, bits[-1])
        early = summed_output(both, [([w_out], 0), (weights[1], 2)], None)
        cores = [([own_core], 0), ([first_core, second_core, half_core], 2)]
        return summed_output(both_core, cores, early)
    if len(far) == 2:
        near[1], far[1] = merge(near[1], far[1]), None
    far = far + [None] * (len(near) - len(far))
    flips = [shared and i == 1 for i in range(len(near))]
    part = partial_output(list(zip(near, far, weights, flips)))
    if not bits:
        return part
    other = swap(part, bits[-1])
    return finish(part, other)


def solution(mesh):
    return jax.shard_map(
        layer,
        mesh=mesh,
        in_specs=(
            P(("grp", "sp"), None),
            P(),
            P(None, "tp"),
            P(None, "tp"),
            P(None, "tp"),
            P("tp", None),
            P("tp", ("grp", "sp")),
        ),
        out_specs=P(("grp", "sp"), None),
        check_vma=False,
    )
```
